512 devices in a mesh: sp: 64 (over z, y), fs: 4 (over x), tp: 2 (over core).
Axes of the slice: x: 4, y: 8, z: 8, core: 2. Of those that a mesh axis runs over, the one named last changes fastest.
Arguments:
- tokens: bfloat16 [4, 24576, 2048], P('fs', ('sp', 'tp')), may hold values from -6 to 6
- norm_gain: float32 [2048], replicated, may hold values from 0.1 to 1.9
- conv_gate_w: bfloat16 [2048, 1024], P('sp', 'tp'), may hold values from -0.125 to 0.125
- conv_in_w: bfloat16 [2048, 1024], P('sp', 'tp'), may hold values from -0.125 to 0.125
- query_w: bfloat16 [2048, 1024], P('sp', 'tp'), may hold values from -0.125 to 0.125
- forget_w: bfloat16 [2048, 1024], P('sp', 'tp'), may hold values from -0.125 to 0.125
- value_w: bfloat16 [2048, 1024], P('sp', 'tp'), may hold values from -0.125 to 0.125
- conv_taps: float32 [3, 1024], P(None, 'tp'), may hold values from -3.5 to 3.5
- floor_gate: float32 [1024], P('tp'), may hold values from 0.93 to 1
- leak: float32 [4, 24576, 8], P('fs', 'sp', 'tp'), may hold values from -1.4 to 0
- head_gain: float32 [128], replicated, may hold values from 0.1 to 1.9
- conv_out_w: bfloat16 [1024, 2048], P('tp', 'fs'), may hold values from -0.125 to 0.125
- chain_out_w: bfloat16 [1024, 2048], P('tp', 'fs'), may hold values from -0.125 to 0.125
Outputs:
- mixed: bfloat16 [4, 24576, 2048], P('fs', ('sp', 'tp'))
The draws below stay inside these ranges and needn't reach their ends.
All inputs are finite; a program needn't handle non-finite values.
Results may differ from the reference program's by a relative error of at most 0.013.
Values may be sent and summed in bfloat16 or wider, within the bound.
No kernel may reach another device: no remote copies, remote signals or barrier semaphores. Data moves between devices by JAX's collectives and lax.ppermute only.
A program may use at most 128 MiB of HBM per device.

```python
import jax
import jax.numpy as jnp
from jax import lax

D = 2048
CW = 1024
HEADS = 8
HEAD_DIM = 128
TOK = 384
BLOCK = 64
HW = 1024
SEQS = 4
LEN = 24576


def draw_floor_gate(key, part):
    base = jax.random.fold_in(key, 101)
    pick_key, fast_key, slow_key = jax.random.split(base, 3)
    fast_share = 0.5
    fast = jax.random.bernoulli(pick_key, fast_share, (HEADS, 1))
    fast_gap = jnp.exp(jax.random.uniform(fast_key, (HEADS, HEAD_DIM), jnp.float32, jnp.log(0.02), jnp.log(0.07)))
    slow_gap = jnp.exp(jax.random.uniform(slow_key, (HEADS, HEAD_DIM), jnp.float32, jnp.log(0.2), jnp.log(0.8))) / LEN
    return (1.0 - jnp.where(fast, fast_gap, slow_gap)).reshape(HEADS * HEAD_DIM).astype(jnp.float32)


def draw_leak(key, part):
    base = jax.random.fold_in(key, 202)
    rate_key, spot_key, depth_key = jax.random.split(base, 3)
    blocks = LEN // TOK
    rates = jnp.exp(jax.random.uniform(rate_key, (SEQS, blocks, 1, HEADS), jnp.float32, jnp.log(0.1), jnp.log(1.0))) / LEN
    constant_fading = -jnp.broadcast_to(rates, (SEQS, blocks, TOK, HEADS)).reshape(SEQS, LEN, HEADS)
    chosen_indices = jax.random.randint(spot_key, (SEQS, 1, HEADS, 2), 0, LEN)
    memory_width = jnp.log(jax.random.uniform(depth_key, (SEQS, 1, HEADS, 2), jnp.float32, 0.5, 0.8))
    sequence_slots = jnp.arange(LEN)[None, :, None, None]
    spike_clusters = jnp.sum(jnp.where(sequence_slots == chosen_indices, memory_width, 0.0), axis=3)
    return (constant_fading + spike_clusters).astype(jnp.float32)


def shard_levels(rng, dims, pieces, least, top_value):
    loudness = 1.0
    for position, parts in pieces:
        steps = jax.random.uniform(jax.random.fold_in(jax.random.fold_in(rng, 6), position), (parts,), jnp.float32, least / len(pieces), top_value / len(pieces))
        loudness = loudness * jnp.repeat(jnp.exp(steps), dims[position] // parts).reshape((-1,) + (1,) * (len(dims) - 1 - position))
    return loudness


def normal_values(stream_key, dims, scale, reach, cuts=(), dtype=jnp.bfloat16):
    values = jax.random.normal(stream_key, dims, jnp.float32) * scale
    if len(cuts) > 0:
        values = shard_levels(stream_key, dims, cuts, -0.22, 0.18) * values
    return jnp.clip(values, min=-reach, max=reach).astype(dtype)


def setup_inputs(seed: int = 0) -> dict:
    key_list = jax.random.split(jax.random.key(seed), 14)
    tokens = normal_values(key_list[0], (SEQS, LEN, D), 1.0, 6.0, ((0, 4), (1, 128)))
    norm_gain = jnp.clip(1.0 + 0.18 * jax.random.normal(key_list[1], (D,), jnp.float32), 0.1, 1.9)
    conv_gate_w = normal_values(key_list[2], (D, CW), D ** -0.5, 0.125, ((0, 64), (1, 2)))
    conv_in_w = normal_values(key_list[3], (D, CW), D ** -0.5, 0.125, ((0, 64), (1, 2)))
    query_w = normal_values(key_list[4], (D, HW), D ** -0.5, 0.125, ((0, 64), (1, 2)))
    forget_w = normal_values(key_list[5], (D, HW), D ** -0.5, 0.125, ((0, 64), (1, 2)))
    value_w = normal_values(key_list[6], (D, HW), D ** -0.5, 0.125, ((0, 64), (1, 2)))
    conv_taps = normal_values(key_list[7], (3, CW), 3 ** -0.5, 3.5, ((1, 2),), jnp.float32)
    floor_gate = draw_floor_gate(jax.random.fold_in(key_list[13], 71), 0)
    leak = draw_leak(jax.random.fold_in(key_list[13], 71), 0)
    head_gain = jnp.clip(1.0 + 0.18 * jax.random.normal(key_list[10], (HEAD_DIM,), jnp.float32), 0.1, 1.9)
    conv_out_w = normal_values(key_list[11], (CW, D), (CW + HW) ** -0.5, 0.125, ((0, 2), (1, 4)))
    chain_out_w = normal_values(key_list[12], (HW, D), (CW + HW) ** -0.5, 0.125, ((0, 2), (1, 4)))
    return {"tokens": tokens, "norm_gain": norm_gain, "conv_gate_w": conv_gate_w, "conv_in_w": conv_in_w, "query_w": query_w, "forget_w": forget_w, "value_w": value_w, "conv_taps": conv_taps, "floor_gate": floor_gate, "leak": leak, "head_gain": head_gain, "conv_out_w": conv_out_w, "chain_out_w": chain_out_w}


HIGH_ACCURACY = lax.Precision.HIGHEST

def norm_rows(matrix, norm_gain):
    values = matrix.astype(jnp.float32)
    center = values - lax.optimization_barrier(jnp.mean(values, axis=-1, keepdims=True))
    spread = lax.optimization_barrier(jnp.mean(center * center, axis=-1, keepdims=True))
    return (center * lax.rsqrt(spread + 1e-05) * norm_gain).astype(jnp.bfloat16)

def block_chain(query, keys, values, decay):
    heads, length, width = query.shape
    count = length // BLOCK

    def split_blocks(array):
        return array.reshape(heads, count, BLOCK, array.shape[-1]).transpose(1, 0, 2, 3)
    causal = jnp.tril(jnp.ones((BLOCK, BLOCK), jnp.float32))

    def advance(hidden_state, inputs):
        query_part, key_portion, value_portion, decay_part = inputs
        running_state = jnp.cumsum(decay_part, axis=1)
        scaled_query = query_part * jnp.exp(running_state)
        key_scaled = key_portion * jnp.exp(-running_state)
        scores = jnp.einsum('htk,hsk->hts', scaled_query, key_scaled, precision=HIGH_ACCURACY) * causal
        inside = jnp.einsum('hts,hsv->htv', scores, value_portion, precision=HIGH_ACCURACY)
        carried_state = jnp.einsum('rgn,rns->rgs', scaled_query, hidden_state, precision=HIGH_ACCURACY)
        final_state = running_state[:, -1:, :]
        state_update = jnp.einsum('qdm,qdt->qmt', key_portion * jnp.exp(final_state - running_state), value_portion, precision=HIGH_ACCURACY)
        return (jnp.exp(final_state[:, 0, :])[:, :, None] * hidden_state + state_update, inside + carried_state)
    initial = jnp.zeros((heads, width, values.shape[-1]), jnp.float32)
    hidden_state, layer_results = lax.scan(advance, initial, (split_blocks(query), split_blocks(keys), split_blocks(values), split_blocks(decay)))
    return (layer_results.transpose(1, 0, 2, 3).reshape(heads, length, values.shape[-1]), hidden_state)

def reference(tokens, norm_gain, conv_gate_w, conv_in_w, query_w, forget_w, value_w, conv_taps, floor_gate, leak, head_gain, conv_out_w, chain_out_w):
    seqs, length, width = tokens.shape
    normed = norm_rows(tokens.reshape(seqs * length, width), norm_gain)

    def project(weight):
        product = jnp.dot(normed, weight, preferred_element_type=jnp.float32)
        return product.astype(jnp.bfloat16).reshape(seqs, length, weight.shape[1])
    second_gate = project(conv_gate_w)
    signal = project(conv_in_w)
    query_raw = project(query_w)
    forget_raw = project(forget_w)
    value_raw = project(value_w)
    margin = conv_taps.shape[0] - 1
    padded = jnp.pad(signal.astype(jnp.float32), ((0, 0), (margin, 0), (0, 0)))
    filtered = jnp.zeros((seqs, length, signal.shape[2]), jnp.float32)
    for offset in range(margin + 1):
        filtered = filtered + conv_taps[offset] * padded[:, offset:offset + length]
    conv_mix = (second_gate.astype(jnp.float32) * filtered).astype(jnp.bfloat16)

    def chain_sequence(inputs):
        query_rows, forget_rows, value_rows, leak_rows = inputs

        def by_head(array):
            return array.astype(jnp.float32).reshape(length, HEADS, HEAD_DIM).transpose(1, 0, 2)
        floor = floor_gate.reshape(HEADS, 1, HEAD_DIM)
        logits = by_head(forget_rows)
        retain = floor + (1.0 - floor) * jax.nn.sigmoid(logits)
        keys = (1.0 - floor) * jax.nn.sigmoid(-logits)
        decay = jnp.log(retain) + leak_rows.T[:, :, None]
        layer_results, _ = block_chain(jax.nn.silu(by_head(query_rows)), keys, by_head(value_rows), decay)
        scale = lax.rsqrt(lax.optimization_barrier(jnp.mean(layer_results * layer_results, axis=-1, keepdims=True)) + 1e-06)
        normal_out = layer_results * scale * head_gain
        return normal_out.transpose(1, 0, 2).reshape(length, HEADS * HEAD_DIM).astype(jnp.bfloat16)
    chain_mix = lax.map(chain_sequence, (query_raw, forget_raw, value_raw, leak))
    mixed = jnp.dot(conv_mix.reshape(seqs * length, -1), conv_out_w, preferred_element_type=jnp.float32)
    mixed = mixed + jnp.dot(chain_mix.reshape(seqs * length, -1), chain_out_w, preferred_element_type=jnp.float32)
    return mixed.astype(jnp.bfloat16).reshape(seqs, length, width)
```

```python
import jax
import jax.numpy as jnp
from jax import lax
from jax.experimental import pallas as pl
from jax.experimental.pallas import tpu as pltpu
from jax.sharding import Mesh
from jax.sharding import PartitionSpec as P

SP = ("sp_0", "sp_1")
SP_TP = ("sp_0", "sp_1", "tp")
F32 = jnp.float32
BF16 = jnp.bfloat16
LANES = 128
SLOT_SHIFT = (0, 3, 1, 2)


def struct(shape, dtype):
    return jax.ShapeDtypeStruct(shape, dtype)


def vmem(count):
    return [pl.BlockSpec(memory_space=pltpu.VMEM) for _ in range(count)]


def split3(values):
    high = values.astype(BF16)
    rest = values - high.astype(F32)
    middle = rest.astype(BF16)
    low = (rest - middle.astype(F32)).astype(BF16)
    return high, middle, low


def dot(a, b, dims=((1,), (0,))):
    return lax.dot_general(a, b, (dims, ((), ())), preferred_element_type=F32)


def norm_kernel(x_ref, gain_ref, o_ref):
    values = x_ref[...].astype(F32)
    center = values - jnp.mean(values, axis=-1, keepdims=True)
    spread = jnp.mean(center * center, axis=-1, keepdims=True)
    o_ref[...] = (center * lax.rsqrt(spread + 1e-05) * gain_ref[...]).astype(BF16)


def norm_rows(tokens, gain):
    return pl.pallas_call(
        norm_kernel,
        out_shape=struct(tokens.shape, BF16),
        in_specs=vmem(2),
        out_specs=vmem(1)[0],
        name="norm",
    )(tokens, gain[None])


def slab_kernel(*refs):
    ins, o_ref = refs[:-1], refs[-1]
    start = pl.multiple_of(lax.axis_index("fs") * LANES, LANES)
    for i, w_ref in enumerate(ins):
        part = w_ref[:, pl.ds(start, LANES)]
        for k in range(o_ref.shape[0]):
            o_ref[k, :, i * LANES : (i + 1) * LANES] = part


def weight_slabs(weights, copies):
    rows = weights[0].shape[0]
    return pl.pallas_call(
        slab_kernel,
        out_shape=struct((copies, rows, len(weights) * LANES), BF16),
        in_specs=vmem(len(weights)),
        out_specs=vmem(1)[0],
        name="slab",
    )(*weights)


def place_rows(scratch, slot, direct, other, w):
    core = lax.axis_index("tp")
    half = direct.shape[0]
    first = pl.multiple_of(core * half, half)
    second = pl.multiple_of((1 - core) * half, half)
    scratch[slot, pl.ds(first, half), :] = dot(direct[...], w).astype(BF16)
    scratch[slot, pl.ds(second, half), :] = dot(other[...], w).astype(BF16)


def lower_triangle(n):
    row = lax.broadcasted_iota(jnp.int32, (n, n), 0)
    col = lax.broadcasted_iota(jnp.int32, (n, n), 1)
    return row >= col


def running_sum(tri, values):
    width = values.shape[1]
    parts = dot(tri, jnp.concatenate(split3(values), axis=1))
    return parts[:, :width] + parts[:, width : 2 * width] + parts[:, 2 * width :]


def state_kernel(*refs):
    toks, (w_ref, floor_ref, *rest) = refs[:8], refs[8:]
    leaks, rest = rest[:4], rest[4:]
    state_ref, run_ref, leak_ref, keys_ref, value_ref, raw = rest
    length = run_ref.shape[1]
    tri = lower_triangle(length).astype(F32).astype(BF16)
    x = lax.axis_index("fs")
    leak_rows = jnp.concatenate(
        [ref[pl.ds(x, 1), :] for ref in leaks] + [jnp.zeros((4, length), F32)], axis=0
    )
    padded = jnp.concatenate([leak_rows, jnp.zeros((LANES - 8, length), F32)], axis=0)
    leak_run = running_sum(tri, padded.T)
    leak_ref[...] = leak_run
    gap = 1.0 - floor_ref[...]
    lane = lax.broadcasted_iota(jnp.int32, (LANES, LANES), 1)
    w = w_ref[...]
    for r in range(4):
        place_rows(raw, r, toks[2 * r], toks[2 * r + 1], w)
        both = raw[r]
        keys = gap * jax.nn.sigmoid(-both[:, :LANES].astype(F32))
        values = both[:, LANES:]
        running = running_sum(tri, jnp.log1p(-keys))
        total = running + leak_run[:, r : r + 1]
        last = total[length - 1 :, :]
        fading = (keys * jnp.exp(last - total)).astype(BF16)
        state = dot(fading, values, ((0,), (0,)))
        spread = jnp.broadcast_to(last, (LANES, LANES)).T
        high = spread.astype(BF16).astype(F32)
        coded = jnp.where(lane < LANES // 2, high, spread - high)
        packed = jnp.concatenate(
            [state.reshape(LANES // 8, 8, LANES), coded.reshape(LANES // 8, 8, LANES)], axis=1
        )
        state_ref[r * 16 : (r + 1) * 16] = packed.astype(BF16)
        run_ref[r] = running
        keys_ref[r] = keys
        value_ref[r] = values


def local_states(toks, w, floor, leaks):
    length = 2 * toks[0].shape[0]
    block = (4, length, LANES)
    return pl.pallas_call(
        state_kernel,
        out_shape=(
            struct((64, 16, LANES), BF16),
            struct(block, F32),
            struct((length, LANES), F32),
            struct(block, F32),
            struct(block, BF16),
        ),
        in_specs=[
            *vmem(8),
            pl.BlockSpec((w.shape[0], 2 * LANES), lambda i: (0, 0)),
            *vmem(5),
        ],
        out_specs=tuple(vmem(5)),
        grid=(1,),
        scratch_shapes=[pltpu.VMEM((4, length, 2 * LANES), BF16)],
        name="states",
    )(*toks, w, floor, *leaks)


def scan_kernel(in_ref, o_ref):
    carry = jnp.zeros((8, LANES), F32)
    for k in range(in_ref.shape[0]):
        both = in_ref[k].astype(F32)
        o_ref[k] = carry.astype(BF16)
        coded = both[8:]
        decay = jnp.exp(coded + pltpu.roll(coded, LANES // 2, 1))
        carry = decay * carry + both[:8]


def scan_blocks(states):
    return pl.pallas_call(
        scan_kernel,
        out_shape=struct((states.shape[0], 8, LANES), BF16),
        in_specs=vmem(1),
        out_specs=vmem(1)[0],
        name="scan",
    )(states)


def inside_kernel(*refs):
    toks, (w_ref, run_ref, leak_ref, keys_ref, value_ref, *rest) = refs[:8], refs[8:]
    inside_ref, reach_ref, gate_ref, signal_ref, raw = rest
    length = run_ref.shape[1]
    causal = lower_triangle(length)
    w = w_ref[...]
    leak_run = leak_ref[...]
    leak_rows = leak_run.T
    for r in range(4):
        place_rows(raw, r, toks[2 * r], toks[2 * r + 1], w)
        gate_ref[r] = raw[r, :, LANES : 2 * LANES]
        signal_ref[r] = raw[r, :, 2 * LANES :]
        running = run_ref[r]
        logits = raw[r, :, :LANES].astype(F32)
        query = logits * jax.nn.sigmoid(logits)
        middle = 0.5 * running[length - 1 :, :]
        ahead = (query * jnp.exp(running - middle)).astype(BF16)
        behind = (keys_ref[r] * jnp.exp(middle - running)).astype(BF16)
        column = leak_run[:, r : r + 1]
        fade = jnp.exp(jnp.where(causal, column - leak_rows[r : r + 1, :], -jnp.inf))
        scores = dot(ahead, behind, ((1,), (1,))) * fade
        inside_ref[r] = dot(scores.astype(BF16), value_ref[r])
        reach_ref[r] = (query * jnp.exp(running + column)).astype(BF16)


def inside_blocks(toks, w, running, leak_run, keys, values):
    length = running.shape[1]
    block = (4, length, LANES)
    return pl.pallas_call(
        inside_kernel,
        out_shape=(struct(block, F32), struct(block, BF16), struct(block, BF16), struct(block, BF16)),
        in_specs=vmem(13),
        out_specs=tuple(vmem(4)),
        scratch_shapes=[pltpu.VMEM((4, length, 3 * LANES), BF16)],
        name="inside",
    )(*toks, w, running, leak_run, keys, values)


def mix_kernel(
    inside_ref, reach_ref, state_ref, gate_ref, signal_ref, rim_ref, taps_ref, gain_ref, o_ref, padded
):
    length = inside_ref.shape[1]
    half = length // 2
    x = lax.axis_index("fs")
    start = pl.multiple_of(x * LANES, LANES)
    taps = taps_ref[:, pl.ds(start, LANES)]
    for r in range(4):
        sequence = (x + SLOT_SHIFT[r]) % 4
        padded[0:8, :] = rim_ref[r, 8:, :].astype(F32)
        padded[8:, :] = signal_ref[r].astype(F32)
        filtered = taps[0:1] * padded[6 : 6 + length, :]
        filtered = filtered + taps[1:2] * padded[7 : 7 + length, :]
        filtered = filtered + taps[2:3] * padded[8 : 8 + length, :]
        conv = (gate_ref[r].astype(F32) * filtered).astype(BF16)
        chain = inside_ref[r] + dot(reach_ref[r], state_ref[r])
        scale = lax.rsqrt(jnp.mean(chain * chain, axis=-1, keepdims=True) + 1e-06)
        chain = (chain * scale * gain_ref[...]).astype(BF16)
        for h in range(2):
            rows = slice(h * half, (h + 1) * half)
            o_ref[2 * sequence + h, :, :LANES] = conv[rows]
            o_ref[2 * sequence + h, :, LANES:] = chain[rows]


def mix_blocks(inside, reach, state, gate, signal, rim, taps, gain):
    length = inside.shape[1]
    return pl.pallas_call(
        mix_kernel,
        out_shape=struct((8, length // 2, 2 * LANES), BF16),
        in_specs=vmem(8),
        out_specs=vmem(1)[0],
        scratch_shapes=[pltpu.VMEM((length + 8, LANES), F32)],
        name="mix",
    )(inside, reach, state, gate, signal, rim, taps, gain)


def out_kernel(mix_ref, *refs):
    w_refs, o_ref = refs[:-1], refs[-1]
    total = jnp.zeros(o_ref.shape, F32)
    for c in range(2):
        lhs = jnp.concatenate(
            [mix_ref[2 * x + c, :, :LANES] for x in range(4)]
            + [mix_ref[2 * x + c, :, LANES:] for x in range(4)],
            axis=1,
        )
        total = total + dot(lhs, w_refs[c][0])
    o_ref[...] = total.astype(BF16)


def out_rows(mix, first, second):
    rows = mix.shape[1]
    pieces, deep, wide = first.shape
    return pl.pallas_call(
        out_kernel,
        out_shape=struct((rows, pieces * wide), BF16),
        grid=(pieces,),
        in_specs=[
            pl.BlockSpec(mix.shape, lambda j: (0, 0, 0)),
            pl.BlockSpec((1, deep, wide), lambda j: (j, 0, 0)),
            pl.BlockSpec((1, deep, wide), lambda j: (j, 0, 0)),
        ],
        out_specs=pl.BlockSpec((rows, wide), lambda j: (0, j)),
        name="out",
    )(mix, first, second)


def ring(array, axis, by):
    count = lax.axis_size(axis)
    return lax.ppermute(array, axis, [(i, (i + by) % count) for i in range(count)])


def exchanged(array, axis):
    return lax.all_to_all(array, axis, split_axis=0, concat_axis=0, tiled=True)


def body(
    tokens,
    norm_gain,
    conv_gate_w,
    conv_in_w,
    query_w,
    forget_w,
    value_w,
    conv_taps,
    floor_gate,
    leak,
    head_gain,
    conv_out_w,
    chain_out_w,
):
    x = lax.axis_index("fs")
    slabs = weight_slabs((forget_w, value_w, query_w, conv_gate_w, conv_in_w), 8)
    y_rows = exchanged(slabs, "sp_1").reshape(-1, slabs.shape[2])
    weights = lax.all_gather(y_rows, "sp_0", axis=0, tiled=True)

    own = norm_rows(tokens[0], norm_gain)
    shifts = (1, 3, 2)
    direct = [own] + [ring(own, "fs", by) for by in shifts]
    other = [ring(part, "tp", 1) for part in direct]
    toks = [part for pair in zip(direct, other) for part in pair]
    own_leak = leak[0].T
    leaks = [own_leak] + [ring(own_leak, "fs", by) for by in shifts]

    out_w = jnp.concatenate([conv_out_w, chain_out_w], axis=0)
    out_w, own = lax.optimization_barrier((out_w, own))
    out_parts = [out_w] + [ring(out_w, "fs", by) for by in shifts]

    floor = lax.dynamic_slice_in_dim(floor_gate, x * LANES, LANES, 0)[None]
    states, running, leak_run, keys, values = local_states(toks, weights, floor, leaks)
    arrived = exchanged(states, SP)
    before = exchanged(scan_blocks(arrived), SP)
    before = before.reshape(4, LANES, LANES)

    inside, reach, gate, signal = inside_blocks(
        toks, weights[:, 2 * LANES :], running, leak_run, keys, values
    )
    count = 64
    tail = signal[:, -16:, :]
    rim = lax.ppermute(tail, SP, [(i, i + 1) for i in range(count - 1)])
    mix = mix_blocks(inside, reach, before, gate, signal, rim, conv_taps, head_gain[None])
    mix = exchanged(mix, ("fs", "tp"))

    slot_of = [SLOT_SHIFT.index(k) for k in range(4)]
    stacked = jnp.stack([out_parts[slot_of[k]] for k in range(4)])
    ordered = jnp.roll(stacked, x, axis=0)
    swapped = ring(ordered, "tp", 1)
    is_first = lax.axis_index("tp") == 0
    first = jnp.where(is_first, ordered, swapped)
    second = jnp.where(is_first, swapped, ordered)
    return out_rows(mix, first, second)[None]


def solution(mesh):
    split = Mesh(
        mesh.devices.reshape(8, 8, mesh.shape["fs"], mesh.shape["tp"]), ("sp_0", "sp_1", "fs", "tp")
    )
    in_specs = (
        P("fs", SP_TP, None),
        P(),
        P(SP, "tp"),
        P(SP, "tp"),
        P(SP, "tp"),
        P(SP, "tp"),
        P(SP, "tp"),
        P(None, "tp"),
        P("tp"),
        P("fs", SP, "tp"),
        P(),
        P("tp", "fs"),
        P("tp", "fs"),
    )
    out_specs = P("fs", SP_TP, None)
    return jax.shard_map(body, mesh=split, in_specs=in_specs, out_specs=out_specs, check_vma=False)
```

```python
import jax
import jax.numpy as jnp
from jax import lax
from jax.experimental import pallas as pl
from jax.experimental.pallas import tpu as pltpu
from jax.sharding import Mesh
from jax.sharding import PartitionSpec as P

SP = ("sp_0", "sp_1")
SP_TP = ("sp_0", "sp_1", "tp")
F32 = jnp.float32
BF16 = jnp.bfloat16
LANES = 128
SLOT_SHIFT = (0, 3, 1, 2)


def struct(shape, dtype):
    return jax.ShapeDtypeStruct(shape, dtype)


def vmem(count):
    return [pl.BlockSpec(memory_space=pltpu.VMEM) for _ in range(count)]


def split3(values):
    high = values.astype(BF16)
    rest = values - high.astype(F32)
    middle = rest.astype(BF16)
    low = (rest - middle.astype(F32)).astype(BF16)
    return high, middle, low


def dot(a, b, dims=((1,), (0,))):
    return lax.dot_general(a, b, (dims, ((), ())), preferred_element_type=F32)


def norm_kernel(x_ref, gain_ref, o_ref):
    values = x_ref[...].astype(F32)
    center = values - jnp.mean(values, axis=-1, keepdims=True)
    spread = jnp.mean(center * center, axis=-1, keepdims=True)
    o_ref[...] = (center * lax.rsqrt(spread + 1e-05) * gain_ref[...]).astype(BF16)


def norm_rows(tokens, gain):
    return pl.pallas_call(
        norm_kernel,
        out_shape=struct(tokens.shape, BF16),
        in_specs=vmem(2),
        out_specs=vmem(1)[0],
        name="norm",
    )(tokens, gain[None])


def slab_kernel(*refs):
    ins, o_ref = refs[:-1], refs[-1]
    start = pl.multiple_of(lax.axis_index("fs") * LANES, LANES)
    for i, w_ref in enumerate(ins):
        part = w_ref[:, pl.ds(start, LANES)]
        for k in range(o_ref.shape[0]):
            o_ref[k, :, i * LANES : (i + 1) * LANES] = part


def weight_slabs(weights, copies):
    rows = weights[0].shape[0]
    return pl.pallas_call(
        slab_kernel,
        out_shape=struct((copies, rows, len(weights) * LANES), BF16),
        in_specs=vmem(len(weights)),
        out_specs=vmem(1)[0],
        name="slab",
    )(*weights)


def copy_kernel(in_ref, o_ref):
    o_ref[...] = in_ref[...]


def passed_on(array):
    return pl.pallas_call(
        copy_kernel,
        out_shape=struct(array.shape, array.dtype),
        in_specs=vmem(1),
        out_specs=vmem(1)[0],
    )(array)


def place_rows(scratch, slot, direct, other, w):
    core = lax.axis_index("tp")
    half = direct.shape[0]
    first = pl.multiple_of(core * half, half)
    second = pl.multiple_of((1 - core) * half, half)
    scratch[slot, pl.ds(first, half), :] = dot(direct[...], w).astype(BF16)
    scratch[slot, pl.ds(second, half), :] = dot(other[...], w).astype(BF16)


def lower_triangle(n):
    row = lax.broadcasted_iota(jnp.int32, (n, n), 0)
    col = lax.broadcasted_iota(jnp.int32, (n, n), 1)
    return row >= col


def running_sum(tri, values):
    width = values.shape[1]
    parts = dot(tri, jnp.concatenate(split3(values), axis=1))
    return parts[:, :width] + parts[:, width : 2 * width] + parts[:, 2 * width :]


def state_kernel(*refs):
    toks, (w_ref, floor_ref, *rest) = refs[:8], refs[8:]
    leaks, rest = rest[:4], rest[4:]
    state_ref, run_ref, leak_ref, keys_ref, value_ref, raw = rest
    length = run_ref.shape[1]
    tri = lower_triangle(length).astype(F32).astype(BF16)
    x = lax.axis_index("fs")
    leak_rows = jnp.concatenate(
        [ref[pl.ds(x, 1), :] for ref in leaks] + [jnp.zeros((4, length), F32)], axis=0
    )
    padded = jnp.concatenate([leak_rows, jnp.zeros((LANES - 8, length), F32)], axis=0)
    leak_run = running_sum(tri, padded.T)
    leak_ref[...] = leak_run
    gap = 1.0 - floor_ref[...]
    lane = lax.broadcasted_iota(jnp.int32, (LANES, LANES), 1)
    w = w_ref[...]
    for r in range(4):
        place_rows(raw, r, toks[2 * r], toks[2 * r + 1], w)
        both = raw[r]
        keys = gap * jax.nn.sigmoid(-both[:, :LANES].astype(F32))
        values = both[:, LANES:]
        running = running_sum(tri, jnp.log1p(-keys))
        total = running + leak_run[:, r : r + 1]
        last = total[length - 1 :, :]
        fading = (keys * jnp.exp(last - total)).astype(BF16)
        state = dot(fading, values, ((0,), (0,)))
        spread = jnp.broadcast_to(last, (LANES, LANES)).T
        high = spread.astype(BF16).astype(F32)
        coded = jnp.where(lane < LANES // 2, high, spread - high)
        packed = jnp.concatenate(
            [state.reshape(LANES // 8, 8, LANES), coded.reshape(LANES // 8, 8, LANES)], axis=1
        )
        state_ref[r * 16 : (r + 1) * 16] = packed.astype(BF16)
        run_ref[r] = running
        keys_ref[r] = keys
        value_ref[r] = values


def local_states(toks, w, floor, leaks):
    length = 2 * toks[0].shape[0]
    block = (4, length, LANES)
    return pl.pallas_call(
        state_kernel,
        out_shape=(
            struct((64, 16, LANES), BF16),
            struct(block, F32),
            struct((length, LANES), F32),
            struct(block, F32),
            struct(block, BF16),
        ),
        in_specs=[
            *vmem(8),
            pl.BlockSpec((w.shape[0], 2 * LANES), lambda i: (0, 0)),
            *vmem(5),
        ],
        out_specs=tuple(vmem(5)),
        grid=(1,),
        scratch_shapes=[pltpu.VMEM((4, length, 2 * LANES), BF16)],
        name="states",
    )(*toks, w, floor, *leaks)


def scan_kernel(in_ref, o_ref):
    carry = jnp.zeros((8, LANES), F32)
    for k in range(in_ref.shape[0]):
        both = in_ref[k].astype(F32)
        o_ref[k] = carry.astype(BF16)
        coded = both[8:]
        decay = jnp.exp(coded + pltpu.roll(coded, LANES // 2, 1))
        carry = decay * carry + both[:8]


def scan_blocks(states):
    return pl.pallas_call(
        scan_kernel,
        out_shape=struct((states.shape[0], 8, LANES), BF16),
        in_specs=vmem(1),
        out_specs=vmem(1)[0],
        name="scan",
    )(states)


def inside_kernel(*refs):
    toks, (w_ref, run_ref, leak_ref, keys_ref, value_ref, *rest) = refs[:8], refs[8:]
    inside_ref, reach_ref, gate_ref, signal_ref, raw = rest
    length = run_ref.shape[1]
    causal = lower_triangle(length)
    w = w_ref[:, 2 * LANES :]
    leak_run = leak_ref[...]
    leak_rows = leak_run.T
    for r in range(4):
        place_rows(raw, r, toks[2 * r], toks[2 * r + 1], w)
        gate_ref[r] = raw[r, :, LANES : 2 * LANES]
        signal_ref[r] = raw[r, :, 2 * LANES :]
        running = run_ref[r]
        logits = raw[r, :, :LANES].astype(F32)
        query = logits * jax.nn.sigmoid(logits)
        middle = 0.5 * running[length - 1 :, :]
        ahead = (query * jnp.exp(running - middle)).astype(BF16)
        behind = (keys_ref[r] * jnp.exp(middle - running)).astype(BF16)
        column = leak_run[:, r : r + 1]
        fade = jnp.exp(jnp.where(causal, column - leak_rows[r : r + 1, :], -jnp.inf))
        scores = dot(ahead, behind, ((1,), (1,))) * fade
        inside_ref[r] = dot(scores.astype(BF16), value_ref[r])
        reach_ref[r] = (query * jnp.exp(running + column)).astype(BF16)


def inside_blocks(toks, w, running, leak_run, keys, values):
    length = running.shape[1]
    block = (4, length, LANES)
    return pl.pallas_call(
        inside_kernel,
        out_shape=(struct(block, F32), struct(block, BF16), struct(block, BF16), struct(block, BF16)),
        in_specs=vmem(13),
        out_specs=tuple(vmem(4)),
        scratch_shapes=[pltpu.VMEM((4, length, 3 * LANES), BF16)],
        name="inside",
    )(*toks, w, running, leak_run, keys, values)


def mix_kernel(
    inside_ref, reach_ref, state_ref, gate_ref, signal_ref, rim_ref, taps_ref, gain_ref, o_ref, padded
):
    length = inside_ref.shape[1]
    half = length // 2
    x = lax.axis_index("fs")
    start = pl.multiple_of(x * LANES, LANES)
    taps = taps_ref[:, pl.ds(start, LANES)]
    for r in range(4):
        sequence = (x + SLOT_SHIFT[r]) % 4
        padded[0:8, :] = rim_ref[r, 8:, :].astype(F32)
        padded[8:, :] = signal_ref[r].astype(F32)
        filtered = taps[0:1] * padded[6 : 6 + length, :]
        filtered = filtered + taps[1:2] * padded[7 : 7 + length, :]
        filtered = filtered + taps[2:3] * padded[8 : 8 + length, :]
        conv = (gate_ref[r].astype(F32) * filtered).astype(BF16)
        chain = inside_ref[r] + dot(reach_ref[r], state_ref[r])
        scale = lax.rsqrt(jnp.mean(chain * chain, axis=-1, keepdims=True) + 1e-06)
        chain = (chain * scale * gain_ref[...]).astype(BF16)
        for h in range(2):
            rows = slice(h * half, (h + 1) * half)
            o_ref[2 * sequence + h, :, :LANES] = conv[rows]
            o_ref[2 * sequence + h, :, LANES:] = chain[rows]


def mix_blocks(inside, reach, state, gate, signal, rim, taps, gain):
    length = inside.shape[1]
    return pl.pallas_call(
        mix_kernel,
        out_shape=struct((8, length // 2, 2 * LANES), BF16),
        in_specs=vmem(8),
        out_specs=vmem(1)[0],
        scratch_shapes=[pltpu.VMEM((length + 8, LANES), F32)],
        name="mix",
    )(inside, reach, state, gate, signal, rim, taps, gain)


def out_kernel(mix_ref, near_ref, far_ref, o_ref):
    core = lax.axis_index("tp")
    total = jnp.zeros(o_ref.shape, F32)
    for c, w_ref in ((core, near_ref), (1 - core, far_ref)):
        pieces = [mix_ref[2 * x + c] for x in range(4)]
        lhs = jnp.concatenate(
            [piece[:, :LANES] for piece in pieces] + [piece[:, LANES:] for piece in pieces], axis=1
        )
        total = total + dot(lhs, w_ref[0])
    o_ref[...] = total.astype(BF16)


def out_rows(mix, near, far):
    rows = mix.shape[1]
    pieces, deep, wide = near.shape
    return pl.pallas_call(
        out_kernel,
        out_shape=struct((rows, pieces * wide), BF16),
        grid=(pieces,),
        in_specs=[
            pl.BlockSpec(mix.shape, lambda j: (0, 0, 0)),
            pl.BlockSpec((1, deep, wide), lambda j: (j, 0, 0)),
            pl.BlockSpec((1, deep, wide), lambda j: (j, 0, 0)),
        ],
        out_specs=pl.BlockSpec((rows, wide), lambda j: (0, j)),
        name="out",
    )(mix, near, far)


def ring(array, axis, by):
    count = lax.axis_size(axis)
    return lax.ppermute(array, axis, [(i, (i + by) % count) for i in range(count)])


def exchanged(array, axis):
    return lax.all_to_all(array, axis, split_axis=0, concat_axis=0, tiled=True)


def layer(
    tokens,
    norm_gain,
    conv_gate_w,
    conv_in_w,
    query_w,
    forget_w,
    value_w,
    conv_taps,
    floor_gate,
    leak,
    head_gain,
    conv_out_w,
    chain_out_w,
):
    x = lax.axis_index("fs")
    slabs = weight_slabs((forget_w, value_w, query_w, conv_gate_w, conv_in_w), 8)
    y_rows = exchanged(slabs, "sp_1").reshape(-1, slabs.shape[2])
    y_rows = passed_on(y_rows)
    weights = lax.all_gather(y_rows, "sp_0", axis=0, tiled=True)

    own = norm_rows(tokens[0], norm_gain)
    own_leak = leak[0].T
    direct, leaks = [own], [own_leak]
    for by in (1, 3, 2):
        direct.append(ring(own, "fs", by))
        leaks.append(ring(own_leak, "fs", by))
    other = []
    for part in direct:
        other.append(ring(part, "tp", 1))
    toks = [part for pair in zip(direct, other) for part in pair]

    out_w = jnp.concatenate([conv_out_w, chain_out_w], axis=0)
    out_w, y_rows = lax.optimization_barrier((out_w, y_rows))
    near = lax.all_gather(out_w, "fs", axis=0)

    floor = lax.dynamic_slice_in_dim(floor_gate, x * LANES, LANES, 0)[None]
    states, running, leak_run, keys, values = local_states(toks, weights, floor, leaks)
    arrived = exchanged(states, SP)
    before = exchanged(scan_blocks(arrived), SP)
    before = before.reshape(4, LANES, LANES)

    inside, reach, gate, signal = inside_blocks(toks, weights, running, leak_run, keys, values)
    count = 64
    tail = signal[:, -16:, :]
    rim = lax.ppermute(tail, SP, [(i, i + 1) for i in range(count - 1)])
    mix = mix_blocks(inside, reach, before, gate, signal, rim, conv_taps, head_gain[None])
    near, mix = lax.optimization_barrier((near, mix))
    mix = exchanged(mix, ("fs", "tp"))
    far = ring(near, "tp", 1)
    return out_rows(mix, near, far)[None]


def solution(mesh):
    split = Mesh(
        mesh.devices.reshape(8, 8, mesh.shape["fs"], mesh.shape["tp"]), ("sp_0", "sp_1", "fs", "tp")
    )
    in_specs = (
        P("fs", SP_TP, None),
        P(),
        P(SP, "tp"),
        P(SP, "tp"),
        P(SP, "tp"),
        P(SP, "tp"),
        P(SP, "tp"),
        P(None, "tp"),
        P("tp"),
        P("fs", SP, "tp"),
        P(),
        P("tp", "fs"),
        P("tp", "fs"),
    )
    out_specs = P("fs", SP_TP, None)
    return jax.shard_map(layer, mesh=split, in_specs=in_specs, out_specs=out_specs, check_vma=False)
```

```python
import jax
import jax.numpy as jnp
from jax import lax
from jax.experimental import pallas as pl
from jax.experimental.pallas import tpu as pltpu
from jax.sharding import Mesh
from jax.sharding import PartitionSpec as P

SP = ("sp_0", "sp_1")
SP_TP = ("sp_0", "sp_1", "tp")
F32 = jnp.float32
BF16 = jnp.bfloat16
LANES = 128


def struct(shape, dtype):
    return jax.ShapeDtypeStruct(shape, dtype)


def vmem(count):
    return [pl.BlockSpec(memory_space=pltpu.VMEM) for _ in range(count)]


def split3(values):
    high = values.astype(BF16)
    rest = values - high.astype(F32)
    middle = rest.astype(BF16)
    low = (rest - middle.astype(F32)).astype(BF16)
    return high, middle, low


def dot(a, b, dims=((1,), (0,))):
    return lax.dot_general(a, b, (dims, ((), ())), preferred_element_type=F32)


def norm_kernel(x_ref, gain_ref, leak_ref, o_ref):
    rows = x_ref.shape[0]
    values = x_ref[...].astype(F32)
    center = values - jnp.mean(values, axis=-1, keepdims=True)
    spread = jnp.mean(center * center, axis=-1, keepdims=True)
    o_ref[:rows, :] = (center * lax.rsqrt(spread + 1e-05) * gain_ref[...]).astype(BF16)
    leaks = jnp.concatenate([leak_ref[h : h + 1, :] for h in range(leak_ref.shape[0])], axis=1)
    parts = [part.astype(F32) for part in split3(leaks)]
    tail = jnp.concatenate([*parts, jnp.zeros((8 - len(parts), leaks.shape[1]), F32)], axis=0)
    unused = jnp.zeros((8, o_ref.shape[1] - leaks.shape[1]), F32)
    o_ref[rows:, :] = jnp.concatenate([tail, unused], axis=1).astype(BF16)


def norm_rows(tokens, gain, leaks):
    return pl.pallas_call(
        norm_kernel,
        out_shape=struct((tokens.shape[0] + 8, tokens.shape[1]), BF16),
        in_specs=vmem(3),
        out_specs=vmem(1)[0],
        name="norm",
    )(tokens, gain[None], leaks)


def slab_kernel(*refs):
    ins, o_ref = refs[:-1], refs[-1]
    start = pl.multiple_of(lax.axis_index("fs") * LANES, LANES)
    both = jnp.concatenate([w_ref[:, pl.ds(start, LANES)] for w_ref in ins], axis=1)
    for k in range(o_ref.shape[0]):
        o_ref[k] = both


def weight_slabs(weights, copies):
    rows = weights[0].shape[0]
    return pl.pallas_call(
        slab_kernel,
        out_shape=struct((copies, rows, len(weights) * LANES), BF16),
        in_specs=vmem(len(weights)),
        out_specs=vmem(1)[0],
        name="slab",
    )(*weights)


def relay_kernel(in_ref, early_ref, late_ref):
    early = in_ref[:, : 2 * LANES]
    for k in range(early_ref.shape[0]):
        early_ref[k] = early
    late_ref[...] = in_ref[:, 2 * LANES :]


def split_columns(rows, copies):
    deep, wide = rows.shape
    return pl.pallas_call(
        relay_kernel,
        out_shape=(
            struct((copies, deep, 2 * LANES), BF16),
            struct((deep, wide - 2 * LANES), BF16),
        ),
        in_specs=vmem(1),
        out_specs=tuple(vmem(2)),
        name="relay",
    )(rows)


def place_rows(scratch, toks, r, w):
    core = lax.axis_index("tp")
    half = scratch.shape[0] // 2
    for part, place in ((2 * r, core), (2 * r + 1, 1 - core)):
        start = pl.multiple_of(place * half, half)
        scratch[pl.ds(start, half), :] = dot(toks[part, :half, :], w).astype(BF16)


def fetches(refs, toks, sems):
    return [pltpu.make_async_copy(ref, toks.at[k], sems.at[k]) for k, ref in enumerate(refs)]


def lower_triangle(n):
    row = lax.broadcasted_iota(jnp.int32, (n, n), 0)
    col = lax.broadcasted_iota(jnp.int32, (n, n), 1)
    return row >= col


def running_sum(tri, values):
    width = values.shape[1]
    parts = dot(tri, jnp.concatenate(split3(values), axis=1))
    return parts[:, :width] + parts[:, width : 2 * width] + parts[:, 2 * width :]


def state_kernel(*refs):
    tok_refs, rest = refs[:8], refs[8:]
    w_ref, floor_ref, state_ref, run_ref, leak_ref, keys_ref, value_ref, raw, toks, sems = rest
    copies = fetches(tok_refs, toks, sems)
    for copy in copies:
        copy.start()
    length = run_ref.shape[1]
    half = length // 2
    tri = lower_triangle(length).astype(F32).astype(BF16)
    gap = 1.0 - floor_ref[...]
    lane = lax.broadcasted_iota(jnp.int32, (LANES, LANES), 1)
    first = pl.multiple_of(lax.axis_index("fs") * length, LANES)
    w = w_ref[...]
    for r in range(4):
        copies[2 * r].wait()
        copies[2 * r + 1].wait()
        coded = toks[2 * r, half:, pl.ds(first, length)].astype(F32)
        leaks = jnp.sum(coded, axis=0, keepdims=True)
        leak_rows = jnp.broadcast_to(leaks, (LANES, length))
        place_rows(raw, toks, r, w)
        keys = gap * jax.nn.sigmoid(-raw[:, :LANES].astype(F32))
        values = raw[:, LANES:]
        both = running_sum(tri, jnp.concatenate([jnp.log1p(-keys), leak_rows.T], axis=1))
        running, leak_run = both[:, :LANES], both[:, LANES:]
        total = running + leak_run
        last = total[length - 1 :, :]
        fading = (keys * jnp.exp(last - total)).astype(BF16)
        state = dot(fading, values, ((0,), (0,)))
        spread = jnp.broadcast_to(last, (LANES, LANES)).T
        high = spread.astype(BF16).astype(F32)
        split = jnp.where(lane < LANES // 2, high, spread - high)
        packed = jnp.concatenate(
            [state.reshape(LANES // 8, 8, LANES), split.reshape(LANES // 8, 8, LANES)], axis=1
        )
        state_ref[r * 16 : (r + 1) * 16] = packed.astype(BF16)
        run_ref[r] = running
        leak_ref[r] = leak_run
        keys_ref[r] = keys
        value_ref[r] = values


def anywhere(count):
    return [pl.BlockSpec(memory_space=pl.ANY) for _ in range(count)]


def token_scratch(tok, columns):
    rows, wide = tok.shape
    return [
        pltpu.VMEM((2 * (rows - 8), columns), BF16),
        pltpu.VMEM((8, rows, wide), BF16),
        pltpu.SemaphoreType.DMA((8,)),
    ]


def local_states(toks, w, floor):
    length = 2 * (toks[0].shape[0] - 8)
    block = (4, length, LANES)
    return pl.pallas_call(
        state_kernel,
        out_shape=(
            struct((64, 16, LANES), BF16),
            struct(block, F32),
            struct(block, F32),
            struct(block, F32),
            struct(block, BF16),
        ),
        in_specs=[*anywhere(8), *vmem(2)],
        out_specs=tuple(vmem(5)),
        scratch_shapes=token_scratch(toks[0], 2 * LANES),
        name="states",
    )(*toks, w, floor)


def sequence_block(*dims):
    return pl.BlockSpec((1, *dims), lambda r: (r, 0, 0))


def whole(*dims):
    return pl.BlockSpec(dims, lambda r: (0,) * len(dims))


def scan_kernel(in_ref, o_ref):
    carry = jnp.zeros((8, LANES), F32)
    for k in range(in_ref.shape[0]):
        both = in_ref[k].astype(F32)
        o_ref[k] = carry.astype(BF16)
        coded = both[8:]
        decay = jnp.exp(coded + pltpu.roll(coded, LANES // 2, 1))
        carry = decay * carry + both[:8]


def scan_blocks(states):
    return pl.pallas_call(
        scan_kernel,
        out_shape=struct((states.shape[0], 8, LANES), BF16),
        in_specs=vmem(1),
        out_specs=vmem(1)[0],
        name="scan",
    )(states)


def inside_kernel(*refs):
    tok_refs, rest = refs[:8], refs[8:]
    w_ref, run_ref, leak_ref, keys_ref, value_ref, *rest = rest
    inside_ref, reach_ref, gate_ref, signal_ref, raw, toks, sems = rest
    copies = fetches(tok_refs, toks, sems)
    for copy in copies:
        copy.start()
    length = run_ref.shape[1]
    causal = lower_triangle(length)
    w = w_ref[...]
    for r in range(4):
        copies[2 * r].wait()
        copies[2 * r + 1].wait()
        place_rows(raw, toks, r, w)
        gate_ref[r] = raw[:, LANES : 2 * LANES]
        signal_ref[r] = raw[:, 2 * LANES :]
        running = run_ref[r]
        leak_run = leak_ref[r]
        logits = raw[:, :LANES].astype(F32)
        query = logits * jax.nn.sigmoid(logits)
        middle = 0.5 * running[length - 1 :, :]
        ahead = (query * jnp.exp(running - middle)).astype(BF16)
        behind = (keys_ref[r] * jnp.exp(middle - running)).astype(BF16)
        fade = jnp.exp(jnp.where(causal, leak_run[:, :1] - leak_run.T[:1, :], -jnp.inf))
        scores = dot(ahead, behind, ((1,), (1,))) * fade
        inside_ref[r] = dot(scores.astype(BF16), value_ref[r])
        reach_ref[r] = (query * jnp.exp(running + leak_run)).astype(BF16)


def inside_blocks(toks, w, running, leak_run, keys, values):
    length = running.shape[1]
    block = (4, length, LANES)
    return pl.pallas_call(
        inside_kernel,
        out_shape=(struct(block, F32), struct(block, BF16), struct(block, BF16), struct(block, BF16)),
        in_specs=[*anywhere(8), *vmem(5)],
        out_specs=tuple(vmem(4)),
        scratch_shapes=token_scratch(toks[0], 3 * LANES),
        name="inside",
    )(*toks, w, running, leak_run, keys, values)


def mix_kernel(
    inside_ref, reach_ref, state_ref, gate_ref, signal_ref, rim_ref, taps_ref, gain_ref, o_ref, padded
):
    length = inside_ref.shape[1]
    half = length // 2
    x = lax.axis_index("fs")
    r = pl.program_id(0)
    shift = jnp.where(r == 1, 3, jnp.where(r == 2, 1, jnp.where(r == 3, 2, 0)))
    sequence = (x + shift) % 4
    start = pl.multiple_of(x * LANES, LANES)
    taps = taps_ref[:, pl.ds(start, LANES)]
    padded[0:8, :] = rim_ref[0, 8:, :].astype(F32)
    padded[8:, :] = signal_ref[0].astype(F32)
    filtered = taps[0:1] * padded[6 : 6 + length, :]
    filtered = filtered + taps[1:2] * padded[7 : 7 + length, :]
    filtered = filtered + taps[2:3] * padded[8 : 8 + length, :]
    conv = (gate_ref[0].astype(F32) * filtered).astype(BF16)
    chain = inside_ref[0] + dot(reach_ref[0], state_ref[0])
    scale = lax.rsqrt(jnp.mean(chain * chain, axis=-1, keepdims=True) + 1e-06)
    chain = (chain * scale * gain_ref[...]).astype(BF16)
    for h in range(2):
        rows = slice(h * half, (h + 1) * half)
        o_ref[2 * sequence + h, :, :LANES] = conv[rows]
        o_ref[2 * sequence + h, :, LANES:] = chain[rows]


def mix_blocks(inside, reach, state, gate, signal, rim, taps, gain):
    length = inside.shape[1]
    narrow = sequence_block(length, LANES)
    return pl.pallas_call(
        mix_kernel,
        out_shape=struct((8, length // 2, 2 * LANES), BF16),
        grid=(4,),
        in_specs=[
            narrow,
            narrow,
            sequence_block(LANES, LANES),
            narrow,
            narrow,
            sequence_block(16, LANES),
            whole(*taps.shape),
            whole(1, LANES),
        ],
        out_specs=whole(8, length // 2, 2 * LANES),
        scratch_shapes=[pltpu.VMEM((length + 8, LANES), F32)],
        name="mix",
    )(inside, reach, state, gate, signal, rim, taps, gain)


def out_kernel(mix_ref, near_ref, far_ref, o_ref):
    core = lax.axis_index("tp")
    total = jnp.zeros(o_ref.shape, F32)
    for c, w_ref in ((core, near_ref), (1 - core, far_ref)):
        pieces = [mix_ref[2 * x + c] for x in range(4)]
        lhs = jnp.concatenate(
            [piece[:, :LANES] for piece in pieces] + [piece[:, LANES:] for piece in pieces], axis=1
        )
        total = total + dot(lhs, w_ref[0])
    o_ref[...] = total.astype(BF16)


def out_rows(mix, near, far):
    rows = mix.shape[1]
    pieces, deep, wide = near.shape
    return pl.pallas_call(
        out_kernel,
        out_shape=struct((rows, pieces * wide), BF16),
        grid=(pieces,),
        in_specs=[whole(*mix.shape), sequence_block(deep, wide), sequence_block(deep, wide)],
        out_specs=pl.BlockSpec((rows, wide), lambda j: (0, j)),
        name="out",
    )(mix, near, far)


def ring(array, axis, by):
    count = lax.axis_size(axis)
    return lax.ppermute(array, axis, [(i, (i + by) % count) for i in range(count)])


def exchanged(array, axis):
    return lax.all_to_all(array, axis, split_axis=0, concat_axis=0, tiled=True)


def layer(
    tokens,
    norm_gain,
    conv_gate_w,
    conv_in_w,
    query_w,
    forget_w,
    value_w,
    conv_taps,
    floor_gate,
    leak,
    head_gain,
    conv_out_w,
    chain_out_w,
):
    x = lax.axis_index("fs")
    slabs = weight_slabs((forget_w, value_w, query_w, conv_gate_w, conv_in_w), 8)
    y_rows = exchanged(slabs, "sp_1").reshape(-1, slabs.shape[2])
    early, late = split_columns(y_rows, 8)
    late_w = lax.all_gather(late, "sp_0", axis=0, tiled=True)
    early_w = exchanged(early, "sp_0").reshape(-1, early.shape[2])

    own = norm_rows(tokens[0], norm_gain, leak[0].T)
    near = [own]
    for by in (1, 3, 2):
        near.append(ring(own, "fs", by))
    far = []
    for part in near:
        far.append(ring(part, "tp", 1))
    toks = [part for pair in zip(near, far) for part in pair]

    out_w = jnp.concatenate([conv_out_w, chain_out_w], axis=0)
    out_w, late = lax.optimization_barrier((out_w, late))
    out_near = lax.all_gather(out_w, "fs", axis=0)
    out_far = ring(out_near, "tp", 1)

    floor = lax.dynamic_slice_in_dim(floor_gate, x * LANES, LANES, 0)[None]
    states, running, leak_run, keys, values = local_states(toks, early_w, floor)
    arrived = exchanged(states, SP)
    before = exchanged(scan_blocks(arrived), SP)
    before = before.reshape(4, LANES, LANES)

    inside, reach, gate, signal = inside_blocks(toks, late_w, running, leak_run, keys, values)
    count = 64
    tail = signal[:, -16:, :]
    rim = lax.ppermute(tail, SP, [(i, i + 1) for i in range(count - 1)])
    mix = mix_blocks(inside, reach, before, gate, signal, rim, conv_taps, head_gain[None])
    mix = exchanged(mix, ("fs", "tp"))
    return out_rows(mix, out_near, out_far)[None]


def solution(mesh):
    split = Mesh(
        mesh.devices.reshape(8, 8, mesh.shape["fs"], mesh.shape["tp"]), ("sp_0", "sp_1", "fs", "tp")
    )
    in_specs = (
        P("fs", SP_TP, None),
        P(),
        P(SP, "tp"),
        P(SP, "tp"),
        P(SP, "tp"),
        P(SP, "tp"),
        P(SP, "tp"),
        P(None, "tp"),
        P("tp"),
        P("fs", SP, "tp"),
        P(),
        P("tp", "fs"),
        P("tp", "fs"),
    )
    out_specs = P("fs", SP_TP, None)
    return jax.shard_map(layer, mesh=split, in_specs=in_specs, out_specs=out_specs, check_vma=False)
```

```python
import jax
import jax.numpy as jnp
from jax import lax
from jax.experimental import pallas as pl
from jax.experimental.pallas import tpu as pltpu
from jax.sharding import Mesh
from jax.sharding import PartitionSpec as P

SP = ("sp_0", "sp_1")
SP_TP = ("sp_0", "sp_1", "tp")
F32 = jnp.float32
BF16 = jnp.bfloat16
LANES = 128
SLOT_SHIFT = (0, 3, 1, 2)


def struct(shape, dtype):
    return jax.ShapeDtypeStruct(shape, dtype)


def vmem(count):
    return [pl.BlockSpec(memory_space=pltpu.VMEM) for _ in range(count)]


def split3(values):
    high = values.astype(BF16)
    rest = values - high.astype(F32)
    middle = rest.astype(BF16)
    low = (rest - middle.astype(F32)).astype(BF16)
    return high, middle, low


def dot(a, b, dims=((1,), (0,))):
    return lax.dot_general(a, b, (dims, ((), ())), preferred_element_type=F32)


def norm_kernel(x_ref, gain_ref, leak_ref, o_ref):
    rows = x_ref.shape[0]
    values = x_ref[...].astype(F32)
    center = values - jnp.mean(values, axis=-1, keepdims=True)
    spread = jnp.mean(center * center, axis=-1, keepdims=True)
    o_ref[:rows, :] = (center * lax.rsqrt(spread + 1e-05) * gain_ref[...]).astype(BF16)
    leaks = jnp.concatenate([leak_ref[h : h + 1, :] for h in range(leak_ref.shape[0])], axis=1)
    parts = [part.astype(F32) for part in split3(leaks)]
    tail = jnp.concatenate([*parts, jnp.zeros((8 - len(parts), leaks.shape[1]), F32)], axis=0)
    unused = jnp.zeros((8, o_ref.shape[1] - leaks.shape[1]), F32)
    o_ref[rows:, :] = jnp.concatenate([tail, unused], axis=1).astype(BF16)


def norm_rows(tokens, gain, leaks):
    return pl.pallas_call(
        norm_kernel,
        out_shape=struct((tokens.shape[0] + 8, tokens.shape[1]), BF16),
        in_specs=vmem(3),
        out_specs=vmem(1)[0],
        name="norm",
    )(tokens, gain[None], leaks)


def slab_kernel(*refs):
    ins, o_ref = refs[:-1], refs[-1]
    start = pl.multiple_of(lax.axis_index("fs") * LANES, LANES)
    both = jnp.concatenate([w_ref[:, pl.ds(start, LANES)] for w_ref in ins], axis=1)
    for k in range(o_ref.shape[0]):
        o_ref[k] = both


def weight_slabs(weights, copies):
    rows = weights[0].shape[0]
    return pl.pallas_call(
        slab_kernel,
        out_shape=struct((copies, rows, len(weights) * LANES), BF16),
        in_specs=vmem(len(weights)),
        out_specs=vmem(1)[0],
        name="slab",
    )(*weights)


def relay_kernel(in_ref, early_ref, late_ref):
    early = in_ref[:, : 2 * LANES]
    for k in range(early_ref.shape[0]):
        early_ref[k] = early
    late_ref[...] = in_ref[:, 2 * LANES :]


def split_columns(rows, copies):
    deep, wide = rows.shape
    return pl.pallas_call(
        relay_kernel,
        out_shape=(
            struct((copies, deep, 2 * LANES), BF16),
            struct((deep, wide - 2 * LANES), BF16),
        ),
        in_specs=vmem(1),
        out_specs=tuple(vmem(2)),
        name="relay",
    )(rows)


def place_rows(scratch, toks, r, w):
    core = lax.axis_index("tp")
    half = scratch.shape[0] // 2
    for part, place in ((2 * r, core), (2 * r + 1, 1 - core)):
        start = pl.multiple_of(place * half, half)
        scratch[pl.ds(start, half), :] = dot(toks[part, :half, :], w).astype(BF16)


def fetches(refs, toks, sems):
    return [pltpu.make_async_copy(ref, toks.at[k], sems.at[k]) for k, ref in enumerate(refs)]


def lower_triangle(n):
    row = lax.broadcasted_iota(jnp.int32, (n, n), 0)
    col = lax.broadcasted_iota(jnp.int32, (n, n), 1)
    return row >= col


def running_sum(tri, values):
    width = values.shape[1]
    parts = dot(tri, jnp.concatenate(split3(values), axis=1))
    return parts[:, :width] + parts[:, width : 2 * width] + parts[:, 2 * width :]


def state_kernel(*refs):
    tok_refs, rest = refs[:8], refs[8:]
    w_ref, floor_ref, state_ref, run_ref, leak_ref, keys_ref, value_ref, raw, toks, sems = rest
    copies = fetches(tok_refs, toks, sems)
    for copy in copies[:4]:
        copy.start()
    length = run_ref.shape[1]
    half = length // 2
    tri = lower_triangle(length).astype(F32).astype(BF16)
    gap = 1.0 - floor_ref[...]
    lane = lax.broadcasted_iota(jnp.int32, (LANES, LANES), 1)
    first = pl.multiple_of(lax.axis_index("fs") * length, LANES)
    w = w_ref[...]
    for r in range(4):
        copies[2 * r].wait()
        copies[2 * r + 1].wait()
        if r < 2:
            copies[2 * r + 4].start()
            copies[2 * r + 5].start()
        coded = toks[2 * r, half:, pl.ds(first, length)].astype(F32)
        leaks = jnp.sum(coded, axis=0, keepdims=True)
        leak_rows = jnp.broadcast_to(leaks, (LANES, length))
        place_rows(raw, toks, r, w)
        keys = gap * jax.nn.sigmoid(-raw[:, :LANES].astype(F32))
        values = raw[:, LANES:]
        both = running_sum(tri, jnp.concatenate([jnp.log1p(-keys), leak_rows.T], axis=1))
        running, leak_run = both[:, :LANES], both[:, LANES:]
        total = running + leak_run
        last = total[length - 1 :, :]
        fading = (keys * jnp.exp(last - total)).astype(BF16)
        state = dot(fading, values, ((0,), (0,)))
        spread = jnp.broadcast_to(last, (LANES, LANES)).T
        high = spread.astype(BF16).astype(F32)
        split = jnp.where(lane < LANES // 2, high, spread - high)
        packed = jnp.concatenate(
            [state.reshape(LANES // 8, 8, LANES), split.reshape(LANES // 8, 8, LANES)], axis=1
        )
        state_ref[r * 16 : (r + 1) * 16] = packed.astype(BF16)
        run_ref[r] = running
        leak_ref[r] = leak_run
        keys_ref[r] = keys
        value_ref[r] = values


def anywhere(count):
    return [pl.BlockSpec(memory_space=pl.ANY) for _ in range(count)]


def token_scratch(tok, columns):
    rows, wide = tok.shape
    return [
        pltpu.VMEM((2 * (rows - 8), columns), BF16),
        pltpu.VMEM((8, rows, wide), BF16),
        pltpu.SemaphoreType.DMA((8,)),
    ]


def local_states(toks, w, floor):
    length = 2 * (toks[0].shape[0] - 8)
    block = (4, length, LANES)
    return pl.pallas_call(
        state_kernel,
        out_shape=(
            struct((64, 16, LANES), BF16),
            struct(block, F32),
            struct(block, F32),
            struct(block, F32),
            struct(block, BF16),
        ),
        in_specs=[*anywhere(8), *vmem(2)],
        out_specs=tuple(vmem(5)),
        scratch_shapes=token_scratch(toks[0], 2 * LANES),
        name="states",
    )(*toks, w, floor)


def sequence_block(*dims):
    return pl.BlockSpec((1, *dims), lambda r: (r, 0, 0))


def whole(*dims):
    return pl.BlockSpec(dims, lambda r: (0,) * len(dims))


def scan_kernel(in_ref, o_ref):
    carry = jnp.zeros((8, LANES), F32)
    for k in range(in_ref.shape[0]):
        both = in_ref[k].astype(F32)
        o_ref[k] = carry.astype(BF16)
        coded = both[8:]
        decay = jnp.exp(coded + pltpu.roll(coded, LANES // 2, 1))
        carry = decay * carry + both[:8]


def scan_blocks(states):
    return pl.pallas_call(
        scan_kernel,
        out_shape=struct((states.shape[0], 8, LANES), BF16),
        in_specs=vmem(1),
        out_specs=vmem(1)[0],
        name="scan",
    )(states)


def inside_kernel(*refs):
    tok_refs, block_refs, rest = refs[:8], refs[8:16], refs[16:]
    run_ref, leak_ref, keys_ref, value_ref, *rest = rest
    inside_ref, reach_ref, gate_ref, signal_ref, raw, toks, sems, weights, weight_sems = rest
    deep = block_refs[0].shape[0]
    z = lax.axis_index("sp_0")
    blocks = []
    for k, ref in enumerate(block_refs):
        start = pl.multiple_of((z + 8 - k) % 8 * deep, deep)
        place = weights.at[pl.ds(start, deep), :]
        blocks.append(pltpu.make_async_copy(ref, place, weight_sems.at[k]))
    copies = fetches(tok_refs, toks, sems)
    for copy in blocks + copies[:4]:
        copy.start()
    length = run_ref.shape[1]
    causal = lower_triangle(length)
    for block in blocks:
        block.wait()
    w = weights[...]
    for r in range(4):
        copies[2 * r].wait()
        copies[2 * r + 1].wait()
        if r < 2:
            copies[2 * r + 4].start()
            copies[2 * r + 5].start()
        place_rows(raw, toks, r, w)
        gate_ref[r] = raw[:, LANES : 2 * LANES]
        signal_ref[r] = raw[:, 2 * LANES :]
        running = run_ref[r]
        leak_run = leak_ref[r]
        logits = raw[:, :LANES].astype(F32)
        query = logits * jax.nn.sigmoid(logits)
        middle = 0.5 * running[length - 1 :, :]
        ahead = (query * jnp.exp(running - middle)).astype(BF16)
        behind = (keys_ref[r] * jnp.exp(middle - running)).astype(BF16)
        fade = jnp.exp(jnp.where(causal, leak_run[:, :1] - leak_run.T[:1, :], -jnp.inf))
        scores = dot(ahead, behind, ((1,), (1,))) * fade
        inside_ref[r] = dot(scores.astype(BF16), value_ref[r])
        reach_ref[r] = (query * jnp.exp(running + leak_run)).astype(BF16)


def inside_blocks(toks, blocks, running, leak_run, keys, values):
    length = running.shape[1]
    block = (4, length, LANES)
    deep, wide = blocks[0].shape
    return pl.pallas_call(
        inside_kernel,
        out_shape=(struct(block, F32), struct(block, BF16), struct(block, BF16), struct(block, BF16)),
        in_specs=[*anywhere(16), *vmem(4)],
        out_specs=tuple(vmem(4)),
        scratch_shapes=[
            *token_scratch(toks[0], wide),
            pltpu.VMEM((8 * deep, wide), BF16),
            pltpu.SemaphoreType.DMA((8,)),
        ],
        name="inside",
    )(*toks, *blocks, running, leak_run, keys, values)


def mix_kernel(
    inside_ref, reach_ref, state_ref, gate_ref, signal_ref, rim_ref, taps_ref, gain_ref, o_ref, padded
):
    length = inside_ref.shape[1]
    half = length // 2
    x = lax.axis_index("fs")
    r = pl.program_id(0)
    shift = jnp.where(r == 1, 3, jnp.where(r == 2, 1, jnp.where(r == 3, 2, 0)))
    sequence = (x + shift) % 4
    start = pl.multiple_of(x * LANES, LANES)
    taps = taps_ref[:, pl.ds(start, LANES)]
    padded[0:8, :] = rim_ref[0, 8:, :].astype(F32)
    padded[8:, :] = signal_ref[0].astype(F32)
    filtered = taps[0:1] * padded[6 : 6 + length, :]
    filtered = filtered + taps[1:2] * padded[7 : 7 + length, :]
    filtered = filtered + taps[2:3] * padded[8 : 8 + length, :]
    conv = (gate_ref[0].astype(F32) * filtered).astype(BF16)
    chain = inside_ref[0] + dot(reach_ref[0], state_ref[0])
    scale = lax.rsqrt(jnp.mean(chain * chain, axis=-1, keepdims=True) + 1e-06)
    chain = (chain * scale * gain_ref[...]).astype(BF16)
    for h in range(2):
        rows = slice(h * half, (h + 1) * half)
        o_ref[2 * sequence + h, :, :LANES] = conv[rows]
        o_ref[2 * sequence + h, :, LANES:] = chain[rows]


def mix_blocks(inside, reach, state, gate, signal, rim, taps, gain):
    length = inside.shape[1]
    narrow = sequence_block(length, LANES)
    return pl.pallas_call(
        mix_kernel,
        out_shape=struct((8, length // 2, 2 * LANES), BF16),
        grid=(4,),
        in_specs=[
            narrow,
            narrow,
            sequence_block(LANES, LANES),
            narrow,
            narrow,
            sequence_block(16, LANES),
            whole(*taps.shape),
            whole(1, LANES),
        ],
        out_specs=whole(8, length // 2, 2 * LANES),
        scratch_shapes=[pltpu.VMEM((length + 8, LANES), F32)],
        name="mix",
    )(inside, reach, state, gate, signal, rim, taps, gain)


def out_kernel(mix_ref, *refs):
    piece_refs, (o_ref, pieces, sems) = refs[:8], refs[8:]
    copies = [pltpu.make_async_copy(ref, pieces.at[k], sems.at[k]) for k, ref in enumerate(piece_refs)]
    for copy in copies[:4]:
        copy.start()
    core = lax.axis_index("tp")
    x = lax.axis_index("fs")
    rows = []
    for c in (core, 1 - core):
        parts = [mix_ref[2 * k + c] for k in range(4)]
        rows.append(
            jnp.concatenate(
                [part[:, :LANES] for part in parts] + [part[:, LANES:] for part in parts], axis=1
            )
        )
    wide = piece_refs[0].shape[1]
    for k in range(4):
        copies[2 * k].wait()
        copies[2 * k + 1].wait()
        if k < 2:
            copies[2 * k + 4].start()
            copies[2 * k + 5].start()
        start = pl.multiple_of((x + SLOT_SHIFT[k]) % 4 * wide, wide)
        total = dot(rows[0], pieces[2 * k]) + dot(rows[1], pieces[2 * k + 1])
        o_ref[:, pl.ds(start, wide)] = total.astype(BF16)


def out_rows(mix, nears, fars):
    rows = mix.shape[1]
    deep, wide = nears[0].shape
    pieces = [piece for pair in zip(nears, fars) for piece in pair]
    return pl.pallas_call(
        out_kernel,
        out_shape=struct((rows, 4 * wide), BF16),
        in_specs=[*vmem(1), *anywhere(8)],
        out_specs=vmem(1)[0],
        scratch_shapes=[pltpu.VMEM((8, deep, wide), BF16), pltpu.SemaphoreType.DMA((8,))],
        name="out",
    )(mix, *pieces)


def ring(array, axis, by):
    count = lax.axis_size(axis)
    return lax.ppermute(array, axis, [(i, (i + by) % count) for i in range(count)])


def exchanged(array, axis):
    return lax.all_to_all(array, axis, split_axis=0, concat_axis=0, tiled=True)


def layer(
    tokens,
    norm_gain,
    conv_gate_w,
    conv_in_w,
    query_w,
    forget_w,
    value_w,
    conv_taps,
    floor_gate,
    leak,
    head_gain,
    conv_out_w,
    chain_out_w,
):
    x = lax.axis_index("fs")
    slabs = weight_slabs((forget_w, value_w, query_w, conv_gate_w, conv_in_w), 8)
    y_rows = exchanged(slabs, "sp_1").reshape(-1, slabs.shape[2])
    early, late = split_columns(y_rows, 8)
    ahead, behind = [late], [late]
    for k in range(1, 5):
        ahead.append(ring(ahead[-1], "sp_0", 1))
        if k < 4:
            behind.append(ring(behind[-1], "sp_0", 7))
    blocks = ahead + behind[:0:-1]
    early_w = exchanged(early, "sp_0").reshape(-1, early.shape[2])

    own = norm_rows(tokens[0], norm_gain, leak[0].T)
    near = [own]
    for by in (1, 3, 2):
        near.append(ring(own, "fs", by))
    far = []
    for part in near:
        far.append(ring(part, "tp", 1))
    toks = [part for pair in zip(near, far) for part in pair]

    out_w = jnp.concatenate([conv_out_w, chain_out_w], axis=0)
    out_near = [out_w]
    for by in (1, 3, 2):
        out_near.append(ring(out_w, "fs", by))
    out_far = []
    for part in out_near:
        out_far.append(ring(part, "tp", 1))

    floor = lax.dynamic_slice_in_dim(floor_gate, x * LANES, LANES, 0)[None]
    states, running, leak_run, keys, values = local_states(toks, early_w, floor)
    arrived = exchanged(states, SP)
    before = exchanged(scan_blocks(arrived), SP)
    before = before.reshape(4, LANES, LANES)

    inside, reach, gate, signal = inside_blocks(toks, blocks, running, leak_run, keys, values)
    count = 64
    tail = signal[:, -16:, :]
    rim = lax.ppermute(tail, SP, [(i, i + 1) for i in range(count - 1)])
    mix = mix_blocks(inside, reach, before, gate, signal, rim, conv_taps, head_gain[None])
    mix = exchanged(mix, ("fs", "tp"))
    return out_rows(mix, out_near, out_far)[None]


def solution(mesh):
    split = Mesh(
        mesh.devices.reshape(8, 8, mesh.shape["fs"], mesh.shape["tp"]), ("sp_0", "sp_1", "fs", "tp")
    )
    in_specs = (
        P("fs", SP_TP, None),
        P(),
        P(SP, "tp"),
        P(SP, "tp"),
        P(SP, "tp"),
        P(SP, "tp"),
        P(SP, "tp"),
        P(None, "tp"),
        P("tp"),
        P("fs", SP, "tp"),
        P(),
        P("tp", "fs"),
        P("tp", "fs"),
    )
    out_specs = P("fs", SP_TP, None)
    return jax.shard_map(layer, mesh=split, in_specs=in_specs, out_specs=out_specs, check_vma=False)
```

```python
import jax
import jax.numpy as jnp
from jax import lax
from jax.experimental import pallas as pl
from jax.experimental.pallas import tpu as pltpu
from jax.sharding import Mesh
from jax.sharding import PartitionSpec as P

SP = ("sp_0", "sp_1")
SP_TP = ("sp_0", "sp_1", "tp")
F32 = jnp.float32
BF16 = jnp.bfloat16
LANES = 128


def struct(shape, dtype):
    return jax.ShapeDtypeStruct(shape, dtype)


def vmem(count):
    return [pl.BlockSpec(memory_space=pltpu.VMEM) for _ in range(count)]


def split_parts(values, count):
    parts = []
    for _ in range(count):
        parts.append(values.astype(BF16))
        values = values - parts[-1].astype(F32)
    return parts


def dot(a, b, dims=((1,), (0,))):
    return lax.dot_general(a, b, (dims, ((), ())), preferred_element_type=F32)


def norm_kernel(x_ref, gain_ref, leak_ref, o_ref):
    rows = x_ref.shape[0]
    values = x_ref[...].astype(F32)
    center = values - jnp.mean(values, axis=-1, keepdims=True)
    spread = jnp.mean(center * center, axis=-1, keepdims=True)
    o_ref[:rows, :] = (center * lax.rsqrt(spread + 1e-05) * gain_ref[...]).astype(BF16)
    heads, length = leak_ref.shape
    parts = [part.astype(F32) for part in split_parts(leak_ref[...], 3)]
    both = jnp.concatenate([*parts, jnp.zeros_like(parts[0])], axis=0).astype(BF16)
    ahead = lax.broadcasted_iota(jnp.int32, (length, length), 0)
    here = lax.broadcasted_iota(jnp.int32, (length, length), 1)
    sums = dot(both, (ahead <= here).astype(F32).astype(BF16))
    total = sums[:heads] + sums[heads : 2 * heads] + sums[2 * heads : 3 * heads]
    leaks = jnp.concatenate([total[h : h + 1, :] for h in range(heads)], axis=1)
    parts = [part.astype(F32) for part in split_parts(leaks, 3)]
    tail = jnp.concatenate([*parts, jnp.zeros((8 - len(parts), leaks.shape[1]), F32)], axis=0)
    unused = jnp.zeros((8, o_ref.shape[1] - leaks.shape[1]), F32)
    o_ref[rows:, :] = jnp.concatenate([tail, unused], axis=1).astype(BF16)


def norm_rows(tokens, gain, leaks):
    return pl.pallas_call(
        norm_kernel,
        out_shape=struct((tokens.shape[0] + 8, tokens.shape[1]), BF16),
        in_specs=vmem(3),
        out_specs=vmem(1)[0],
        name="norm",
    )(tokens, gain[None], leaks)


def slab_kernel(*refs):
    ins, o_ref = refs[:-1], refs[-1]
    start = pl.multiple_of(lax.axis_index("fs") * LANES, LANES)
    both = jnp.concatenate([w_ref[:, pl.ds(start, LANES)] for w_ref in ins], axis=1)
    for k in range(o_ref.shape[0]):
        o_ref[k] = both


def weight_slabs(weights, copies):
    rows = weights[0].shape[0]
    return pl.pallas_call(
        slab_kernel,
        out_shape=struct((copies, rows, len(weights) * LANES), BF16),
        in_specs=vmem(len(weights)),
        out_specs=vmem(1)[0],
        name="slab",
    )(*weights)


def relay_kernel(in_ref, o_ref):
    o_ref[...] = in_ref[...]


def relayed(rows):
    return pl.pallas_call(
        relay_kernel,
        out_shape=struct(rows.shape, rows.dtype),
        in_specs=vmem(1),
        out_specs=vmem(1)[0],
        compiler_params=pltpu.CompilerParams(vmem_limit_bytes=2 << 20),
        name="relay",
    )(rows)


def place_rows(scratch, toks, r, w):
    core = lax.axis_index("tp")
    half = scratch.shape[0] // 2
    for part, place in ((2 * r, core), (2 * r + 1, 1 - core)):
        start = pl.multiple_of(place * half, half)
        scratch[pl.ds(start, half), :] = dot(toks[part, :half, :], w).astype(BF16)


def fetches(refs, toks, sems):
    return [pltpu.make_async_copy(ref, toks.at[k], sems.at[k]) for k, ref in enumerate(refs)]


def lower_triangle(n):
    row = lax.broadcasted_iota(jnp.int32, (n, n), 0)
    col = lax.broadcasted_iota(jnp.int32, (n, n), 1)
    return row >= col


def gates(logits, gap, tri):
    keys = gap * jax.nn.sigmoid(-logits.astype(F32))
    parts = dot(tri, jnp.concatenate(split_parts(jnp.log1p(-keys), 2), axis=1))
    return keys, parts[:, :LANES] + parts[:, LANES:]


def leak_row(toks, r, length):
    first = pl.multiple_of(lax.axis_index("fs") * length, LANES)
    coded = toks[2 * r, length // 2 :, pl.ds(first, length)].astype(F32)
    return jnp.sum(coded, axis=0, keepdims=True)


def state_kernel(*refs):
    tok_refs, rest = refs[:8], refs[8:]
    w_ref, floor_ref, state_ref, raw_ref, toks, sems, weights, w_sem = rest
    w_copy = pltpu.make_async_copy(w_ref.at[:, : 2 * LANES], weights, w_sem)
    copies = fetches(tok_refs, toks, sems)
    for copy in [w_copy] + copies[:4]:
        copy.start()
    length = raw_ref.shape[1]
    tri = lower_triangle(length).astype(F32).astype(BF16)
    gap = 1.0 - floor_ref[...]
    lane = lax.broadcasted_iota(jnp.int32, (LANES, LANES), 1)
    w_copy.wait()
    w = weights[...]
    for r in range(4):
        copies[2 * r].wait()
        copies[2 * r + 1].wait()
        if r < 2:
            copies[2 * r + 4].start()
            copies[2 * r + 5].start()
        place_rows(raw_ref.at[r], toks, r, w)
        keys, running = gates(raw_ref[r, :, :LANES], gap, tri)
        leaks = jnp.broadcast_to(leak_row(toks, r, length), (LANES, length))
        total = running + leaks.T
        last = total[length - 1 :, :]
        fading = (keys * jnp.exp(last - total)).astype(BF16)
        state = dot(fading, raw_ref[r, :, LANES:], ((0,), (0,)))
        spread = jnp.broadcast_to(last, (LANES, LANES)).T
        high = spread.astype(BF16).astype(F32)
        split = jnp.where(lane < LANES // 2, high, spread - high)
        packed = jnp.concatenate(
            [state.reshape(LANES // 8, 8, LANES), split.reshape(LANES // 8, 8, LANES)], axis=1
        )
        state_ref[r * 16 : (r + 1) * 16] = packed.astype(BF16)


def anywhere(count):
    return [pl.BlockSpec(memory_space=pl.ANY) for _ in range(count)]


def token_scratch(tok, deep, columns):
    return [
        pltpu.VMEM((8, *tok.shape), BF16),
        pltpu.SemaphoreType.DMA((8,)),
        pltpu.VMEM((deep, columns), BF16),
        pltpu.SemaphoreType.DMA,
    ]


def local_states(toks, w, floor):
    length = 2 * (toks[0].shape[0] - 8)
    return pl.pallas_call(
        state_kernel,
        out_shape=(struct((64, 16, LANES), BF16), struct((4, length, 2 * LANES), BF16)),
        in_specs=[*anywhere(9), *vmem(1)],
        out_specs=tuple(vmem(2)),
        scratch_shapes=token_scratch(toks[0], w.shape[0], 2 * LANES),
        name="states",
    )(*toks, w, floor)


def sequence_block(*dims):
    return pl.BlockSpec((1, *dims), lambda r: (r, 0, 0))


def whole(*dims):
    return pl.BlockSpec(dims, lambda r: (0,) * len(dims))


def scan_kernel(in_ref, o_ref):
    carry = jnp.zeros((8, LANES), F32)
    for k in range(in_ref.shape[0]):
        both = in_ref[k].astype(F32)
        o_ref[k] = carry.astype(BF16)
        coded = both[8:]
        decay = jnp.exp(coded + pltpu.roll(coded, LANES // 2, 1))
        carry = decay * carry + both[:8]


def scan_blocks(states):
    return pl.pallas_call(
        scan_kernel,
        out_shape=struct((states.shape[0], 8, LANES), BF16),
        in_specs=vmem(1),
        out_specs=vmem(1)[0],
        compiler_params=pltpu.CompilerParams(vmem_limit_bytes=4 << 20),
        name="scan",
    )(states)


def inside_kernel(*refs):
    tok_refs, rest = refs[:8], refs[8:]
    w_ref, floor_ref, early_ref, *rest = rest
    inside_ref, reach_ref, gate_ref, signal_ref, toks, sems, weights, w_sem, raw = rest
    w_copy = pltpu.make_async_copy(w_ref.at[:, 2 * LANES :], weights, w_sem)
    copies = fetches(tok_refs, toks, sems)
    for copy in [w_copy] + copies[:4]:
        copy.start()
    length = early_ref.shape[1]
    causal = lower_triangle(length)
    tri = causal.astype(F32).astype(BF16)
    gap = 1.0 - floor_ref[...]
    w_copy.wait()
    w = weights[...]
    for r in range(4):
        keys, running = gates(early_ref[r, :, :LANES], gap, tri)
        copies[2 * r].wait()
        copies[2 * r + 1].wait()
        if r < 2:
            copies[2 * r + 4].start()
            copies[2 * r + 5].start()
        place_rows(raw, toks, r, w)
        gate_ref[r] = raw[:, LANES : 2 * LANES]
        signal_ref[r] = raw[:, 2 * LANES :]
        logits = raw[:, :LANES].astype(F32)
        query = logits * jax.nn.sigmoid(logits)
        middle = 0.5 * running[length - 1 :, :]
        ahead = (query * jnp.exp(running - middle)).astype(BF16)
        behind = (keys * jnp.exp(middle - running)).astype(BF16)
        leaks = leak_row(toks, r, length)
        columns = jnp.broadcast_to(leaks, (LANES, length)).T
        fade = jnp.exp(jnp.where(causal, columns[:, :1] - leaks, -jnp.inf))
        scores = dot(ahead, behind, ((1,), (1,))) * fade
        inside_ref[r] = dot(scores.astype(BF16), early_ref[r, :, LANES:])
        reach_ref[r] = (query * jnp.exp(running + columns)).astype(BF16)


def inside_blocks(toks, w, floor, early):
    length = early.shape[1]
    block = (4, length, LANES)
    return pl.pallas_call(
        inside_kernel,
        out_shape=(struct(block, F32), struct(block, BF16), struct(block, BF16), struct(block, BF16)),
        in_specs=[*anywhere(9), *vmem(2)],
        out_specs=tuple(vmem(4)),
        scratch_shapes=[
            *token_scratch(toks[0], w.shape[0], 3 * LANES),
            pltpu.VMEM((length, 3 * LANES), BF16),
        ],
        name="inside",
    )(*toks, w, floor, early)


def mix_kernel(
    inside_ref, reach_ref, state_ref, gate_ref, signal_ref, rim_ref, taps_ref, gain_ref, o_ref, padded
):
    length = inside_ref.shape[1]
    half = length // 2
    x = lax.axis_index("fs")
    r = pl.program_id(0)
    shift = jnp.where(r == 1, 3, jnp.where(r == 2, 1, jnp.where(r == 3, 2, 0)))
    sequence = (x + shift) % 4
    start = pl.multiple_of(x * LANES, LANES)
    taps = taps_ref[:, pl.ds(start, LANES)]
    padded[0:8, :] = rim_ref[0, 8:, :].astype(F32)
    padded[8:, :] = signal_ref[0].astype(F32)
    filtered = taps[0:1] * padded[6 : 6 + length, :]
    filtered = filtered + taps[1:2] * padded[7 : 7 + length, :]
    filtered = filtered + taps[2:3] * padded[8 : 8 + length, :]
    conv = (gate_ref[0].astype(F32) * filtered).astype(BF16)
    chain = inside_ref[0] + dot(reach_ref[0], state_ref[0])
    scale = lax.rsqrt(jnp.mean(chain * chain, axis=-1, keepdims=True) + 1e-06)
    chain = (chain * scale * gain_ref[...]).astype(BF16)
    for h in range(2):
        rows = slice(h * half, (h + 1) * half)
        o_ref[2 * sequence + h, :, :LANES] = conv[rows]
        o_ref[2 * sequence + h, :, LANES:] = chain[rows]


def mix_blocks(inside, reach, state, gate, signal, rim, taps, gain):
    length = inside.shape[1]
    narrow = sequence_block(length, LANES)
    return pl.pallas_call(
        mix_kernel,
        out_shape=struct((8, length // 2, 2 * LANES), BF16),
        grid=(4,),
        in_specs=[
            narrow,
            narrow,
            sequence_block(LANES, LANES),
            narrow,
            narrow,
            sequence_block(16, LANES),
            whole(*taps.shape),
            whole(1, LANES),
        ],
        out_specs=whole(8, length // 2, 2 * LANES),
        scratch_shapes=[pltpu.VMEM((length + 8, LANES), F32)],
        name="mix",
    )(inside, reach, state, gate, signal, rim, taps, gain)


def out_kernel(mix_ref, near_ref, far_ref, o_ref):
    core = lax.axis_index("tp")
    total = jnp.zeros(o_ref.shape, F32)
    for c, w_ref in ((core, near_ref), (1 - core, far_ref)):
        pieces = [mix_ref[2 * x + c] for x in range(4)]
        lhs = jnp.concatenate(
            [piece[:, :LANES] for piece in pieces] + [piece[:, LANES:] for piece in pieces], axis=1
        )
        total = total + dot(lhs, w_ref[0])
    o_ref[...] = total.astype(BF16)


def out_rows(mix, near, far):
    rows = mix.shape[1]
    pieces, deep, wide = near.shape
    return pl.pallas_call(
        out_kernel,
        out_shape=struct((rows, pieces * wide), BF16),
        grid=(pieces,),
        in_specs=[whole(*mix.shape), sequence_block(deep, wide), sequence_block(deep, wide)],
        out_specs=pl.BlockSpec((rows, wide), lambda j: (0, j)),
        name="out",
    )(mix, near, far)


def ring(array, axis, by):
    count = lax.axis_size(axis)
    return lax.ppermute(array, axis, [(i, (i + by) % count) for i in range(count)])


def exchanged(array, axis):
    return lax.all_to_all(array, axis, split_axis=0, concat_axis=0, tiled=True)


def layer(
    tokens,
    norm_gain,
    conv_gate_w,
    conv_in_w,
    query_w,
    forget_w,
    value_w,
    conv_taps,
    floor_gate,
    leak,
    head_gain,
    conv_out_w,
    chain_out_w,
):
    x = lax.axis_index("fs")
    slabs = weight_slabs((forget_w, value_w, query_w, conv_gate_w, conv_in_w), 8)
    y_rows = exchanged(slabs, "sp_1").reshape(-1, slabs.shape[2])
    y_rows = relayed(y_rows)
    weights = lax.all_gather(y_rows, "sp_0", axis=0, tiled=True)

    own = norm_rows(tokens[0], norm_gain, leak[0].T)
    near = [own]
    for by in (1, 3, 2):
        near.append(ring(own, "fs", by))
    far = []
    for part in near:
        far.append(ring(part, "tp", 1))
    toks = [part for pair in zip(near, far) for part in pair]

    out_w = jnp.concatenate([conv_out_w, chain_out_w], axis=0)
    out_w, y_rows = lax.optimization_barrier((out_w, y_rows))
    out_near = lax.all_gather(out_w, "fs", axis=0)
    out_far = ring(out_near, "tp", 1)

    floor = lax.dynamic_slice_in_dim(floor_gate, x * LANES, LANES, 0)[None]
    states, early = local_states(toks, weights, floor)
    arrived = exchanged(states, SP)
    before = exchanged(scan_blocks(arrived), SP)
    before = before.reshape(4, LANES, LANES)

    inside, reach, gate, signal = inside_blocks(toks, weights, floor, early)
    count = 64
    tail = signal[:, -16:, :]
    rim = lax.ppermute(tail, SP, [(i, i + 1) for i in range(count - 1)])
    mix = mix_blocks(inside, reach, before, gate, signal, rim, conv_taps, head_gain[None])
    mix = exchanged(mix, ("fs", "tp"))
    return out_rows(mix, out_near, out_far)[None]


def solution(mesh):
    split = Mesh(
        mesh.devices.reshape(8, 8, mesh.shape["fs"], mesh.shape["tp"]), ("sp_0", "sp_1", "fs", "tp")
    )
    in_specs = (
        P("fs", SP_TP, None),
        P(),
        P(SP, "tp"),
        P(SP, "tp"),
        P(SP, "tp"),
        P(SP, "tp"),
        P(SP, "tp"),
        P(None, "tp"),
        P("tp"),
        P("fs", SP, "tp"),
        P(),
        P("tp", "fs"),
        P("tp", "fs"),
    )
    out_specs = P("fs", SP_TP, None)
    return jax.shard_map(layer, mesh=split, in_specs=in_specs, out_specs=out_specs, check_vma=False)
```

```python
import jax
import jax.numpy as jnp
from jax import lax
from jax.experimental import pallas as pl
from jax.experimental.pallas import tpu as pltpu
from jax.sharding import Mesh
from jax.sharding import PartitionSpec as P

SP = ("sp_0", "sp_1")
SP_TP = ("sp_0", "sp_1", "tp")
F32 = jnp.float32
BF16 = jnp.bfloat16
LANES = 128


def struct(shape, dtype):
    return jax.ShapeDtypeStruct(shape, dtype)


def vmem(count):
    return [pl.BlockSpec(memory_space=pltpu.VMEM) for _ in range(count)]


def split_parts(values, count):
    parts = []
    for _ in range(count):
        parts.append(values.astype(BF16))
        values = values - parts[-1].astype(F32)
    return parts


def dot(a, b, dims=((1,), (0,))):
    return lax.dot_general(a, b, (dims, ((), ())), preferred_element_type=F32)


def norm_kernel(x_ref, gain_ref, leak_ref, o_ref):
    rows = x_ref.shape[0]
    values = x_ref[...].astype(F32)
    center = values - jnp.mean(values, axis=-1, keepdims=True)
    spread = jnp.mean(center * center, axis=-1, keepdims=True)
    o_ref[:rows, :] = (center * lax.rsqrt(spread + 1e-05) * gain_ref[...]).astype(BF16)
    heads, length = leak_ref.shape
    parts = [part.astype(F32) for part in split_parts(leak_ref[...], 3)]
    both = jnp.concatenate([*parts, jnp.zeros_like(parts[0])], axis=0).astype(BF16)
    ahead = lax.broadcasted_iota(jnp.int32, (length, length), 0)
    here = lax.broadcasted_iota(jnp.int32, (length, length), 1)
    sums = dot(both, (ahead <= here).astype(F32).astype(BF16))
    total = sums[:heads] + sums[heads : 2 * heads] + sums[2 * heads : 3 * heads]
    leaks = jnp.concatenate([total[h : h + 1, :] for h in range(heads)], axis=1)
    parts = [part.astype(F32) for part in split_parts(leaks, 3)]
    tail = jnp.concatenate([*parts, jnp.zeros((8 - len(parts), leaks.shape[1]), F32)], axis=0)
    unused = jnp.zeros((8, o_ref.shape[1] - leaks.shape[1]), F32)
    o_ref[rows:, :] = jnp.concatenate([tail, unused], axis=1).astype(BF16)


def norm_rows(tokens, gain, leaks):
    return pl.pallas_call(
        norm_kernel,
        out_shape=struct((tokens.shape[0] + 8, tokens.shape[1]), BF16),
        in_specs=vmem(3),
        out_specs=vmem(1)[0],
        name="norm",
    )(tokens, gain[None], leaks)


def slab_kernel(*refs):
    ins, o_ref = refs[:-1], refs[-1]
    start = pl.multiple_of(lax.axis_index("fs") * LANES, LANES)
    both = jnp.concatenate([w_ref[:, pl.ds(start, LANES)] for w_ref in ins], axis=1)
    for k in range(o_ref.shape[0]):
        o_ref[k] = both


def weight_slabs(weights, copies):
    rows = weights[0].shape[0]
    return pl.pallas_call(
        slab_kernel,
        out_shape=struct((copies, rows, len(weights) * LANES), BF16),
        in_specs=vmem(len(weights)),
        out_specs=vmem(1)[0],
        name="slab",
    )(*weights)


def relay_kernel(in_ref, o_ref):
    o_ref[...] = in_ref[...]


def relayed(rows):
    return pl.pallas_call(
        relay_kernel,
        out_shape=struct(rows.shape, rows.dtype),
        in_specs=vmem(1),
        out_specs=vmem(1)[0],
        compiler_params=pltpu.CompilerParams(vmem_limit_bytes=2 << 20),
        name="relay",
    )(rows)


def place_rows(out, toks, r, w):
    core = lax.axis_index("tp")
    half = out.shape[0] // 2
    both = jnp.concatenate([toks[2 * r, :half, :], toks[2 * r + 1, :half, :]], axis=0)
    result = dot(both, w).astype(BF16)
    first = pl.multiple_of(core * half, half)
    second = pl.multiple_of((1 - core) * half, half)
    out[pl.ds(first, half), :] = result[:half]
    out[pl.ds(second, half), :] = result[half:]


def fetches(refs, toks, sems):
    return [pltpu.make_async_copy(ref, toks.at[k], sems.at[k]) for k, ref in enumerate(refs)]


def lower_triangle(n):
    row = lax.broadcasted_iota(jnp.int32, (n, n), 0)
    col = lax.broadcasted_iota(jnp.int32, (n, n), 1)
    return row >= col


def gates(logits, gap, tri):
    keys = gap * jax.nn.sigmoid(-logits.astype(F32))
    parts = dot(tri, jnp.concatenate(split_parts(jnp.log1p(-keys), 2), axis=1))
    return keys, parts[:, :LANES] + parts[:, LANES:]


def leak_row(toks, r, length):
    first = pl.multiple_of(lax.axis_index("fs") * length, LANES)
    coded = toks[2 * r, length // 2 :, pl.ds(first, length)].astype(F32)
    return jnp.sum(coded, axis=0, keepdims=True)


def state_kernel(*refs):
    tok_refs, rest = refs[:8], refs[8:]
    w_ref, floor_ref, state_ref, raw_ref, toks, sems, weights, w_sem = rest
    w_copy = pltpu.make_async_copy(w_ref.at[:, : 2 * LANES], weights, w_sem)
    copies = fetches(tok_refs, toks, sems)
    for copy in [w_copy] + copies[:4]:
        copy.start()
    length = raw_ref.shape[1]
    tri = lower_triangle(length).astype(F32).astype(BF16)
    gap = 1.0 - floor_ref[...]
    lane = lax.broadcasted_iota(jnp.int32, (LANES, LANES), 1)
    w_copy.wait()
    w = weights[...]
    for r in range(4):
        copies[2 * r].wait()
        copies[2 * r + 1].wait()
        if r < 2:
            copies[2 * r + 4].start()
            copies[2 * r + 5].start()
        place_rows(raw_ref.at[r], toks, r, w)
        keys, running = gates(raw_ref[r, :, :LANES], gap, tri)
        leaks = jnp.broadcast_to(leak_row(toks, r, length), (LANES, length))
        total = running + leaks.T
        last = total[length - 1 :, :]
        fading = (keys * jnp.exp(last - total)).astype(BF16)
        state = dot(fading, raw_ref[r, :, LANES:], ((0,), (0,)))
        spread = jnp.broadcast_to(last, (LANES, LANES)).T
        high = spread.astype(BF16).astype(F32)
        split = jnp.where(lane < LANES // 2, high, spread - high)
        packed = jnp.concatenate(
            [state.reshape(LANES // 8, 8, LANES), split.reshape(LANES // 8, 8, LANES)], axis=1
        )
        state_ref[r * 16 : (r + 1) * 16] = packed.astype(BF16)


def anywhere(count):
    return [pl.BlockSpec(memory_space=pl.ANY) for _ in range(count)]


def token_scratch(tok, deep, columns):
    return [
        pltpu.VMEM((8, *tok.shape), BF16),
        pltpu.SemaphoreType.DMA((8,)),
        pltpu.VMEM((deep, columns), BF16),
        pltpu.SemaphoreType.DMA,
    ]


def local_states(toks, w, floor):
    length = 2 * (toks[0].shape[0] - 8)
    return pl.pallas_call(
        state_kernel,
        out_shape=(struct((64, 16, LANES), BF16), struct((4, length, 2 * LANES), BF16)),
        in_specs=[*anywhere(9), *vmem(1)],
        out_specs=tuple(vmem(2)),
        scratch_shapes=token_scratch(toks[0], w.shape[0], 2 * LANES),
        name="states",
    )(*toks, w, floor)


def sequence_block(*dims):
    return pl.BlockSpec((1, *dims), lambda r: (r, 0, 0))


def whole(*dims):
    return pl.BlockSpec(dims, lambda r: (0,) * len(dims))


def scan_kernel(in_ref, o_ref):
    carry = jnp.zeros((8, LANES), F32)
    for k in range(in_ref.shape[0]):
        both = in_ref[k].astype(F32)
        o_ref[k] = carry.astype(BF16)
        coded = both[8:]
        decay = jnp.exp(coded + pltpu.roll(coded, LANES // 2, 1))
        carry = decay * carry + both[:8]


def scan_blocks(states):
    return pl.pallas_call(
        scan_kernel,
        out_shape=struct((states.shape[0], 8, LANES), BF16),
        in_specs=vmem(1),
        out_specs=vmem(1)[0],
        compiler_params=pltpu.CompilerParams(vmem_limit_bytes=4 << 20),
        name="scan",
    )(states)


def inside_kernel(*refs):
    tok_refs, rest = refs[:8], refs[8:]
    w_ref, floor_ref, early_ref, *rest = rest
    inside_ref, reach_ref, gate_ref, signal_ref, toks, sems, weights, w_sem, raw = rest
    w_copy = pltpu.make_async_copy(w_ref.at[:, 2 * LANES :], weights, w_sem)
    copies = fetches(tok_refs, toks, sems)
    for copy in [w_copy] + copies[:4]:
        copy.start()
    length = early_ref.shape[1]
    causal = lower_triangle(length)
    tri = causal.astype(F32).astype(BF16)
    gap = 1.0 - floor_ref[...]
    w_copy.wait()
    w = weights[...]
    for r in range(4):
        keys, running = gates(early_ref[r, :, :LANES], gap, tri)
        copies[2 * r].wait()
        copies[2 * r + 1].wait()
        if r < 2:
            copies[2 * r + 4].start()
            copies[2 * r + 5].start()
        place_rows(raw, toks, r, w)
        gate_ref[r] = raw[:, LANES : 2 * LANES]
        signal_ref[r] = raw[:, 2 * LANES :]
        logits = raw[:, :LANES].astype(F32)
        query = logits * jax.nn.sigmoid(logits)
        middle = 0.5 * running[length - 1 :, :]
        ahead = (query * jnp.exp(running - middle)).astype(BF16)
        behind = (keys * jnp.exp(middle - running)).astype(BF16)
        leaks = leak_row(toks, r, length)
        columns = jnp.broadcast_to(leaks, (LANES, length)).T
        fade = jnp.exp(jnp.where(causal, columns[:, :1] - leaks, -jnp.inf))
        scores = dot(ahead, behind, ((1,), (1,))) * fade
        inside_ref[r] = dot(scores.astype(BF16), early_ref[r, :, LANES:])
        reach_ref[r] = (query * jnp.exp(running + columns)).astype(BF16)


def inside_blocks(toks, w, floor, early):
    length = early.shape[1]
    block = (4, length, LANES)
    return pl.pallas_call(
        inside_kernel,
        out_shape=(struct(block, F32), struct(block, BF16), struct(block, BF16), struct(block, BF16)),
        in_specs=[*anywhere(9), *vmem(2)],
        out_specs=tuple(vmem(4)),
        scratch_shapes=[
            *token_scratch(toks[0], w.shape[0], 3 * LANES),
            pltpu.VMEM((length, 3 * LANES), BF16),
        ],
        name="inside",
    )(*toks, w, floor, early)


def mix_kernel(
    inside_ref, reach_ref, state_ref, gate_ref, signal_ref, rim_ref, taps_ref, gain_ref, o_ref, padded
):
    length = inside_ref.shape[1]
    half = length // 2
    x = lax.axis_index("fs")
    r = pl.program_id(0)
    shift = jnp.where(r == 1, 3, jnp.where(r == 2, 1, jnp.where(r == 3, 2, 0)))
    sequence = (x + shift) % 4
    start = pl.multiple_of(x * LANES, LANES)
    taps = taps_ref[:, pl.ds(start, LANES)]
    padded[0:8, :] = rim_ref[0, 8:, :].astype(F32)
    padded[8:, :] = signal_ref[0].astype(F32)
    filtered = taps[0:1] * padded[6 : 6 + length, :]
    filtered = filtered + taps[1:2] * padded[7 : 7 + length, :]
    filtered = filtered + taps[2:3] * padded[8 : 8 + length, :]
    conv = (gate_ref[0].astype(F32) * filtered).astype(BF16)
    chain = inside_ref[0] + dot(reach_ref[0], state_ref[0])
    scale = lax.rsqrt(jnp.mean(chain * chain, axis=-1, keepdims=True) + 1e-06)
    chain = (chain * scale * gain_ref[...]).astype(BF16)
    for h in range(2):
        rows = slice(h * half, (h + 1) * half)
        o_ref[2 * sequence + h, :, :LANES] = conv[rows]
        o_ref[2 * sequence + h, :, LANES:] = chain[rows]


def mix_blocks(inside, reach, state, gate, signal, rim, taps, gain):
    length = inside.shape[1]
    narrow = sequence_block(length, LANES)
    return pl.pallas_call(
        mix_kernel,
        out_shape=struct((8, length // 2, 2 * LANES), BF16),
        grid=(4,),
        in_specs=[
            narrow,
            narrow,
            sequence_block(LANES, LANES),
            narrow,
            narrow,
            sequence_block(16, LANES),
            whole(*taps.shape),
            whole(1, LANES),
        ],
        out_specs=whole(8, length // 2, 2 * LANES),
        scratch_shapes=[pltpu.VMEM((length + 8, LANES), F32)],
        name="mix",
    )(inside, reach, state, gate, signal, rim, taps, gain)


def out_kernel(mix_ref, near_ref, far_ref, o_ref, near, sems):
    copies = [pltpu.make_async_copy(near_ref.at[x], near.at[x], sems.at[x]) for x in range(4)]
    for copy in copies:
        copy.start()
    core = lax.axis_index("tp")
    rows = []
    for c in (core, 1 - core):
        pieces = [mix_ref[2 * x + c] for x in range(4)]
        rows.append(
            jnp.concatenate(
                [piece[:, :LANES] for piece in pieces] + [piece[:, LANES:] for piece in pieces],
                axis=1,
            )
        )
    wide = near_ref.shape[2]
    for x in range(4):
        total = dot(rows[1], far_ref[x])
        copies[x].wait()
        total = total + dot(rows[0], near[x])
        o_ref[:, x * wide : (x + 1) * wide] = total.astype(BF16)


def out_rows(mix, near, far):
    rows = mix.shape[1]
    pieces, _, wide = near.shape
    return pl.pallas_call(
        out_kernel,
        out_shape=struct((rows, pieces * wide), BF16),
        in_specs=[*vmem(1), *anywhere(1), *vmem(1)],
        out_specs=vmem(1)[0],
        scratch_shapes=[pltpu.VMEM(near.shape, BF16), pltpu.SemaphoreType.DMA((4,))],
        compiler_params=pltpu.CompilerParams(vmem_limit_bytes=20 << 20),
        name="out",
    )(mix, near, far)


def ring(array, axis, by):
    count = lax.axis_size(axis)
    return lax.ppermute(array, axis, [(i, (i + by) % count) for i in range(count)])


def exchanged(array, axis):
    return lax.all_to_all(array, axis, split_axis=0, concat_axis=0, tiled=True)


def layer(
    tokens,
    norm_gain,
    conv_gate_w,
    conv_in_w,
    query_w,
    forget_w,
    value_w,
    conv_taps,
    floor_gate,
    leak,
    head_gain,
    conv_out_w,
    chain_out_w,
):
    x = lax.axis_index("fs")
    slabs = weight_slabs((forget_w, value_w, query_w, conv_gate_w, conv_in_w), 8)
    y_rows = exchanged(slabs, "sp_1").reshape(-1, slabs.shape[2])
    y_rows = relayed(y_rows)
    weights = lax.all_gather(y_rows, "sp_0", axis=0, tiled=True)

    own = norm_rows(tokens[0], norm_gain, leak[0].T)
    near = [own]
    for by in (1, 3, 2):
        near.append(ring(own, "fs", by))
    far = []
    for part in near:
        far.append(ring(part, "tp", 1))
    toks = [part for pair in zip(near, far) for part in pair]

    out_w = jnp.concatenate([conv_out_w, chain_out_w], axis=0)
    out_w, y_rows = lax.optimization_barrier((out_w, y_rows))
    out_near = lax.all_gather(out_w, "fs", axis=0)
    out_far = ring(out_near, "tp", 1)

    floor = lax.dynamic_slice_in_dim(floor_gate, x * LANES, LANES, 0)[None]
    states, early = local_states(toks, weights, floor)
    arrived = exchanged(states, SP)
    before = exchanged(scan_blocks(arrived), SP)
    before = before.reshape(4, LANES, LANES)

    inside, reach, gate, signal = inside_blocks(toks, weights, floor, early)
    count = 64
    tail = signal[:, -16:, :]
    rim = lax.ppermute(tail, SP, [(i, i + 1) for i in range(count - 1)])
    mix = mix_blocks(inside, reach, before, gate, signal, rim, conv_taps, head_gain[None])
    mix = exchanged(mix, ("fs", "tp"))
    return out_rows(mix, out_near, out_far)[None]


def solution(mesh):
    split = Mesh(
        mesh.devices.reshape(8, 8, mesh.shape["fs"], mesh.shape["tp"]), ("sp_0", "sp_1", "fs", "tp")
    )
    in_specs = (
        P("fs", SP_TP, None),
        P(),
        P(SP, "tp"),
        P(SP, "tp"),
        P(SP, "tp"),
        P(SP, "tp"),
        P(SP, "tp"),
        P(None, "tp"),
        P("tp"),
        P("fs", SP, "tp"),
        P(),
        P("tp", "fs"),
        P("tp", "fs"),
    )
    out_specs = P("fs", SP_TP, None)
    return jax.shard_map(layer, mesh=split, in_specs=in_specs, out_specs=out_specs, check_vma=False)
```

```python
import jax
import jax.numpy as jnp
from jax import lax
from jax.experimental import pallas as pl
from jax.experimental.pallas import tpu as pltpu
from jax.sharding import Mesh
from jax.sharding import PartitionSpec as P

SP = ("sp_0", "sp_1")
SP_TP = ("sp_0", "sp_1", "tp")
F32 = jnp.float32
BF16 = jnp.bfloat16
LANES = 128
SLOT_SHIFT = (0, 3, 1, 2)


def struct(shape, dtype):
    return jax.ShapeDtypeStruct(shape, dtype)


def vmem(count):
    return [pl.BlockSpec(memory_space=pltpu.VMEM) for _ in range(count)]


def split_parts(values, count):
    parts = []
    for _ in range(count):
        parts.append(values.astype(BF16))
        values = values - parts[-1].astype(F32)
    return parts


def dot(a, b, dims=((1,), (0,))):
    return lax.dot_general(a, b, (dims, ((), ())), preferred_element_type=F32)


def norm_kernel(x_ref, gain_ref, leak_ref, o_ref):
    rows = x_ref.shape[0]
    values = x_ref[...].astype(F32)
    center = values - jnp.mean(values, axis=-1, keepdims=True)
    spread = jnp.mean(center * center, axis=-1, keepdims=True)
    o_ref[:rows, :] = (center * lax.rsqrt(spread + 1e-05) * gain_ref[...]).astype(BF16)
    heads, length = leak_ref.shape
    parts = [part.astype(F32) for part in split_parts(leak_ref[...], 3)]
    both = jnp.concatenate([*parts, jnp.zeros_like(parts[0])], axis=0).astype(BF16)
    ahead = lax.broadcasted_iota(jnp.int32, (length, length), 0)
    here = lax.broadcasted_iota(jnp.int32, (length, length), 1)
    sums = dot(both, (ahead <= here).astype(F32).astype(BF16))
    total = sums[:heads] + sums[heads : 2 * heads] + sums[2 * heads : 3 * heads]
    leaks = jnp.concatenate([total[h : h + 1, :] for h in range(heads)], axis=1)
    parts = [part.astype(F32) for part in split_parts(leaks, 3)]
    tail = jnp.concatenate([*parts, jnp.zeros((8 - len(parts), leaks.shape[1]), F32)], axis=0)
    unused = jnp.zeros((8, o_ref.shape[1] - leaks.shape[1]), F32)
    o_ref[rows:, :] = jnp.concatenate([tail, unused], axis=1).astype(BF16)


def norm_rows(tokens, gain, leaks):
    return pl.pallas_call(
        norm_kernel,
        out_shape=struct((tokens.shape[0] + 8, tokens.shape[1]), BF16),
        in_specs=vmem(3),
        out_specs=vmem(1)[0],
        name="norm",
    )(tokens, gain[None], leaks)


def slab_kernel(*refs):
    ins, o_ref = refs[:-1], refs[-1]
    start = pl.multiple_of(lax.axis_index("fs") * LANES, LANES)
    both = jnp.concatenate([w_ref[:, pl.ds(start, LANES)] for w_ref in ins], axis=1)
    for k in range(o_ref.shape[0]):
        o_ref[k] = both


def weight_slabs(weights, copies):
    rows = weights[0].shape[0]
    return pl.pallas_call(
        slab_kernel,
        out_shape=struct((copies, rows, len(weights) * LANES), BF16),
        in_specs=vmem(len(weights)),
        out_specs=vmem(1)[0],
        name="slab",
    )(*weights)


def relay_kernel(in_ref, early_ref, late_ref):
    early = in_ref[:, : 2 * LANES]
    for k in range(early_ref.shape[0]):
        early_ref[k] = early
    late_ref[...] = in_ref[:, 2 * LANES :]


def split_columns(rows, copies):
    deep, wide = rows.shape
    return pl.pallas_call(
        relay_kernel,
        out_shape=(
            struct((copies, deep, 2 * LANES), BF16),
            struct((deep, wide - 2 * LANES), BF16),
        ),
        in_specs=vmem(1),
        out_specs=tuple(vmem(2)),
        compiler_params=pltpu.CompilerParams(vmem_limit_bytes=4 << 20),
        name="relay",
    )(rows)


def place_rows(scratch, toks, r, w):
    core = lax.axis_index("tp")
    half = scratch.shape[0] // 2
    for part, place in ((2 * r, core), (2 * r + 1, 1 - core)):
        start = pl.multiple_of(place * half, half)
        scratch[pl.ds(start, half), :] = dot(toks[part, :half, :], w).astype(BF16)


def fetches(refs, toks, sems):
    return [pltpu.make_async_copy(ref, toks.at[k], sems.at[k]) for k, ref in enumerate(refs)]


def lower_triangle(n):
    row = lax.broadcasted_iota(jnp.int32, (n, n), 0)
    col = lax.broadcasted_iota(jnp.int32, (n, n), 1)
    return row >= col


def gates(logits, gap, tri):
    keys = gap * jax.nn.sigmoid(-logits.astype(F32))
    parts = dot(tri, jnp.concatenate(split_parts(jnp.log1p(-keys), 2), axis=1))
    return keys, parts[:, :LANES] + parts[:, LANES:]


def leak_row(toks, r, length):
    first = pl.multiple_of(lax.axis_index("fs") * length, LANES)
    coded = toks[2 * r, length // 2 :, pl.ds(first, length)].astype(F32)
    return jnp.sum(coded, axis=0, keepdims=True)


def state_kernel(*refs):
    tok_refs, rest = refs[:8], refs[8:]
    w_ref, floor_ref, state_ref, raw_ref, toks, sems, weights, w_sem = rest
    w_copy = pltpu.make_async_copy(w_ref, weights, w_sem)
    copies = fetches(tok_refs, toks, sems)
    for copy in [w_copy] + copies[:4]:
        copy.start()
    length = raw_ref.shape[1]
    tri = lower_triangle(length).astype(F32).astype(BF16)
    gap = 1.0 - floor_ref[...]
    lane = lax.broadcasted_iota(jnp.int32, (LANES, LANES), 1)
    w_copy.wait()
    w = weights[...]
    for r in range(4):
        copies[2 * r].wait()
        copies[2 * r + 1].wait()
        if r < 2:
            copies[2 * r + 4].start()
            copies[2 * r + 5].start()
        place_rows(raw_ref.at[r], toks, r, w)
        keys, running = gates(raw_ref[r, :, :LANES], gap, tri)
        leaks = jnp.broadcast_to(leak_row(toks, r, length), (LANES, length))
        total = running + leaks.T
        last = total[length - 1 :, :]
        fading = (keys * jnp.exp(last - total)).astype(BF16)
        state = dot(fading, raw_ref[r, :, LANES:], ((0,), (0,)))
        spread = jnp.broadcast_to(last, (LANES, LANES)).T
        high = spread.astype(BF16).astype(F32)
        split = jnp.where(lane < LANES // 2, high, spread - high)
        packed = jnp.concatenate(
            [state.reshape(LANES // 8, 8, LANES), split.reshape(LANES // 8, 8, LANES)], axis=1
        )
        state_ref[r * 16 : (r + 1) * 16] = packed.astype(BF16)


def anywhere(count):
    return [pl.BlockSpec(memory_space=pl.ANY) for _ in range(count)]


def token_scratch(tok, deep, columns):
    return [
        pltpu.VMEM((8, *tok.shape), BF16),
        pltpu.SemaphoreType.DMA((8,)),
        pltpu.VMEM((deep, columns), BF16),
        pltpu.SemaphoreType.DMA,
    ]


def local_states(toks, w, floor):
    length = 2 * (toks[0].shape[0] - 8)
    return pl.pallas_call(
        state_kernel,
        out_shape=(struct((64, 16, LANES), BF16), struct((4, length, 2 * LANES), BF16)),
        in_specs=[*anywhere(9), *vmem(1)],
        out_specs=tuple(vmem(2)),
        scratch_shapes=token_scratch(toks[0], w.shape[0], 2 * LANES),
        name="states",
    )(*toks, w, floor)


def sequence_block(*dims):
    return pl.BlockSpec((1, *dims), lambda r: (r, 0, 0))


def whole(*dims):
    return pl.BlockSpec(dims, lambda r: (0,) * len(dims))


def scan_kernel(in_ref, o_ref):
    carry = jnp.zeros((8, LANES), F32)
    for k in range(in_ref.shape[0]):
        both = in_ref[k].astype(F32)
        o_ref[k] = carry.astype(BF16)
        coded = both[8:]
        decay = jnp.exp(coded + pltpu.roll(coded, LANES // 2, 1))
        carry = decay * carry + both[:8]


def scan_blocks(states):
    return pl.pallas_call(
        scan_kernel,
        out_shape=struct((states.shape[0], 8, LANES), BF16),
        in_specs=vmem(1),
        out_specs=vmem(1)[0],
        compiler_params=pltpu.CompilerParams(vmem_limit_bytes=4 << 20),
        name="scan",
    )(states)


def inside_kernel(*refs):
    tok_refs, rest = refs[:8], refs[8:]
    w_ref, floor_ref, early_ref, *rest = rest
    inside_ref, reach_ref, gate_ref, signal_ref, toks, sems, weights, w_sem, raw = rest
    w_copy = pltpu.make_async_copy(w_ref, weights, w_sem)
    copies = fetches(tok_refs, toks, sems)
    for copy in [w_copy] + copies[:4]:
        copy.start()
    length = early_ref.shape[1]
    causal = lower_triangle(length)
    tri = causal.astype(F32).astype(BF16)
    gap = 1.0 - floor_ref[...]
    w_copy.wait()
    w = weights[...]
    for r in range(4):
        keys, running = gates(early_ref[r, :, :LANES], gap, tri)
        copies[2 * r].wait()
        copies[2 * r + 1].wait()
        if r < 2:
            copies[2 * r + 4].start()
            copies[2 * r + 5].start()
        place_rows(raw, toks, r, w)
        gate_ref[r] = raw[:, LANES : 2 * LANES]
        signal_ref[r] = raw[:, 2 * LANES :]
        logits = raw[:, :LANES].astype(F32)
        query = logits * jax.nn.sigmoid(logits)
        middle = 0.5 * running[length - 1 :, :]
        ahead = (query * jnp.exp(running - middle)).astype(BF16)
        behind = (keys * jnp.exp(middle - running)).astype(BF16)
        leaks = leak_row(toks, r, length)
        columns = jnp.broadcast_to(leaks, (LANES, length)).T
        fade = jnp.exp(jnp.where(causal, columns[:, :1] - leaks, -jnp.inf))
        scores = dot(ahead, behind, ((1,), (1,))) * fade
        inside_ref[r] = dot(scores.astype(BF16), early_ref[r, :, LANES:])
        reach_ref[r] = (query * jnp.exp(running + columns)).astype(BF16)


def inside_blocks(toks, w, floor, early):
    length = early.shape[1]
    block = (4, length, LANES)
    return pl.pallas_call(
        inside_kernel,
        out_shape=(struct(block, F32), struct(block, BF16), struct(block, BF16), struct(block, BF16)),
        in_specs=[*anywhere(9), *vmem(2)],
        out_specs=tuple(vmem(4)),
        scratch_shapes=[
            *token_scratch(toks[0], w.shape[0], 3 * LANES),
            pltpu.VMEM((length, 3 * LANES), BF16),
        ],
        name="inside",
    )(*toks, w, floor, early)


def mix_kernel(
    inside_ref, reach_ref, state_ref, gate_ref, signal_ref, rim_ref, taps_ref, gain_ref, o_ref, padded
):
    length = inside_ref.shape[1]
    half = length // 2
    x = lax.axis_index("fs")
    r = pl.program_id(0)
    shift = jnp.where(r == 1, 3, jnp.where(r == 2, 1, jnp.where(r == 3, 2, 0)))
    sequence = (x + shift) % 4
    start = pl.multiple_of(x * LANES, LANES)
    taps = taps_ref[:, pl.ds(start, LANES)]
    padded[0:8, :] = rim_ref[0, 8:, :].astype(F32)
    padded[8:, :] = signal_ref[0].astype(F32)
    filtered = taps[0:1] * padded[6 : 6 + length, :]
    filtered = filtered + taps[1:2] * padded[7 : 7 + length, :]
    filtered = filtered + taps[2:3] * padded[8 : 8 + length, :]
    conv = (gate_ref[0].astype(F32) * filtered).astype(BF16)
    chain = inside_ref[0] + dot(reach_ref[0], state_ref[0])
    scale = lax.rsqrt(jnp.mean(chain * chain, axis=-1, keepdims=True) + 1e-06)
    chain = (chain * scale * gain_ref[...]).astype(BF16)
    for h in range(2):
        rows = slice(h * half, (h + 1) * half)
        o_ref[2 * sequence + h, :, :LANES] = conv[rows]
        o_ref[2 * sequence + h, :, LANES:] = chain[rows]


def mix_blocks(inside, reach, state, gate, signal, rim, taps, gain):
    length = inside.shape[1]
    narrow = sequence_block(length, LANES)
    return pl.pallas_call(
        mix_kernel,
        out_shape=struct((8, length // 2, 2 * LANES), BF16),
        grid=(4,),
        in_specs=[
            narrow,
            narrow,
            sequence_block(LANES, LANES),
            narrow,
            narrow,
            sequence_block(16, LANES),
            whole(*taps.shape),
            whole(1, LANES),
        ],
        out_specs=whole(8, length // 2, 2 * LANES),
        scratch_shapes=[pltpu.VMEM((length + 8, LANES), F32)],
        name="mix",
    )(inside, reach, state, gate, signal, rim, taps, gain)


def out_kernel(mix_ref, *refs):
    piece_refs, (o_ref, pieces, sems) = refs[:8], refs[8:]
    copies = [pltpu.make_async_copy(ref, pieces.at[k], sems.at[k]) for k, ref in enumerate(piece_refs)]
    for copy in copies[:4]:
        copy.start()
    core = lax.axis_index("tp")
    x = lax.axis_index("fs")
    rows = []
    for c in (core, 1 - core):
        parts = [mix_ref[2 * k + c] for k in range(4)]
        rows.append(
            jnp.concatenate(
                [part[:, :LANES] for part in parts] + [part[:, LANES:] for part in parts], axis=1
            )
        )
    wide = piece_refs[0].shape[1]
    for k in range(4):
        copies[2 * k].wait()
        copies[2 * k + 1].wait()
        if k < 2:
            copies[2 * k + 4].start()
            copies[2 * k + 5].start()
        start = pl.multiple_of((x + SLOT_SHIFT[k]) % 4 * wide, wide)
        total = dot(rows[0], pieces[2 * k]) + dot(rows[1], pieces[2 * k + 1])
        o_ref[:, pl.ds(start, wide)] = total.astype(BF16)


def out_rows(mix, nears, fars):
    rows = mix.shape[1]
    deep, wide = nears[0].shape
    pieces = [piece for pair in zip(nears, fars) for piece in pair]
    return pl.pallas_call(
        out_kernel,
        out_shape=struct((rows, 4 * wide), BF16),
        in_specs=[*vmem(1), *anywhere(8)],
        out_specs=vmem(1)[0],
        scratch_shapes=[pltpu.VMEM((8, deep, wide), BF16), pltpu.SemaphoreType.DMA((8,))],
        name="out",
    )(mix, *pieces)


def ring(array, axis, by):
    count = lax.axis_size(axis)
    return lax.ppermute(array, axis, [(i, (i + by) % count) for i in range(count)])


def exchanged(array, axis):
    return lax.all_to_all(array, axis, split_axis=0, concat_axis=0, tiled=True)


def layer(
    tokens,
    norm_gain,
    conv_gate_w,
    conv_in_w,
    query_w,
    forget_w,
    value_w,
    conv_taps,
    floor_gate,
    leak,
    head_gain,
    conv_out_w,
    chain_out_w,
):
    x = lax.axis_index("fs")
    slabs = weight_slabs((forget_w, value_w, query_w, conv_gate_w, conv_in_w), 8)
    y_rows = exchanged(slabs, "sp_1").reshape(-1, slabs.shape[2])
    early, late = split_columns(y_rows, 8)
    early_w = exchanged(early, "sp_0").reshape(-1, early.shape[2])
    late_w = lax.all_gather(late, "sp_0", axis=0, tiled=True)

    own = norm_rows(tokens[0], norm_gain, leak[0].T)
    near = [own]
    for by in (1, 3, 2):
        near.append(ring(own, "fs", by))
    far = []
    for part in near:
        far.append(ring(part, "tp", 1))
    toks = [part for pair in zip(near, far) for part in pair]

    out_w = jnp.concatenate([conv_out_w, chain_out_w], axis=0)
    out_near = [out_w]
    for by in (1, 3, 2):
        out_near.append(ring(out_w, "fs", by))
    out_far = []
    for part in out_near:
        out_far.append(ring(part, "tp", 1))

    floor = lax.dynamic_slice_in_dim(floor_gate, x * LANES, LANES, 0)[None]
    states, projected = local_states(toks, early_w, floor)
    arrived = exchanged(states, SP)
    before = exchanged(scan_blocks(arrived), SP)
    before = before.reshape(4, LANES, LANES)

    inside, reach, gate, signal = inside_blocks(toks, late_w, floor, projected)
    count = 64
    tail = signal[:, -16:, :]
    rim = lax.ppermute(tail, SP, [(i, i + 1) for i in range(count - 1)])
    mix = mix_blocks(inside, reach, before, gate, signal, rim, conv_taps, head_gain[None])
    mix = exchanged(mix, ("fs", "tp"))
    return out_rows(mix, out_near, out_far)[None]


def solution(mesh):
    split = Mesh(
        mesh.devices.reshape(8, 8, mesh.shape["fs"], mesh.shape["tp"]), ("sp_0", "sp_1", "fs", "tp")
    )
    in_specs = (
        P("fs", SP_TP, None),
        P(),
        P(SP, "tp"),
        P(SP, "tp"),
        P(SP, "tp"),
        P(SP, "tp"),
        P(SP, "tp"),
        P(None, "tp"),
        P("tp"),
        P("fs", SP, "tp"),
        P(),
        P("tp", "fs"),
        P("tp", "fs"),
    )
    out_specs = P("fs", SP_TP, None)
    return jax.shard_map(layer, mesh=split, in_specs=in_specs, out_specs=out_specs, check_vma=False)
```

```python
import jax
import jax.numpy as jnp
from jax import lax
from jax.experimental import pallas as pl
from jax.experimental.pallas import tpu as pltpu
from jax.sharding import Mesh
from jax.sharding import PartitionSpec as P

SP = ("sp_0", "sp_1")
SP_TP = ("sp_0", "sp_1", "tp")
F32 = jnp.float32
BF16 = jnp.bfloat16
LANES = 128
SLOT_SHIFT = (0, 3, 1, 2)


def struct(shape, dtype):
    return jax.ShapeDtypeStruct(shape, dtype)


def vmem(count):
    return [pl.BlockSpec(memory_space=pltpu.VMEM) for _ in range(count)]


def split_parts(values, count):
    parts = []
    for _ in range(count):
        parts.append(values.astype(BF16))
        values = values - parts[-1].astype(F32)
    return parts


def dot(a, b, dims=((1,), (0,))):
    return lax.dot_general(a, b, (dims, ((), ())), preferred_element_type=F32)


def norm_kernel(x_ref, gain_ref, leak_ref, o_ref):
    rows = x_ref.shape[0]
    values = x_ref[...].astype(F32)
    center = values - jnp.mean(values, axis=-1, keepdims=True)
    spread = jnp.mean(center * center, axis=-1, keepdims=True)
    o_ref[:rows, :] = (center * lax.rsqrt(spread + 1e-05) * gain_ref[...]).astype(BF16)
    heads, length = leak_ref.shape
    parts = [part.astype(F32) for part in split_parts(leak_ref[...], 3)]
    both = jnp.concatenate([*parts, jnp.zeros_like(parts[0])], axis=0).astype(BF16)
    ahead = lax.broadcasted_iota(jnp.int32, (length, length), 0)
    here = lax.broadcasted_iota(jnp.int32, (length, length), 1)
    sums = dot(both, (ahead <= here).astype(F32).astype(BF16))
    total = sums[:heads] + sums[heads : 2 * heads] + sums[2 * heads : 3 * heads]
    leaks = jnp.concatenate([total[h : h + 1, :] for h in range(heads)], axis=1)
    parts = [part.astype(F32) for part in split_parts(leaks, 3)]
    tail = jnp.concatenate([*parts, jnp.zeros((8 - len(parts), leaks.shape[1]), F32)], axis=0)
    unused = jnp.zeros((8, o_ref.shape[1] - leaks.shape[1]), F32)
    o_ref[rows:, :] = jnp.concatenate([tail, unused], axis=1).astype(BF16)


def norm_rows(tokens, gain, leaks):
    return pl.pallas_call(
        norm_kernel,
        out_shape=struct((tokens.shape[0] + 8, tokens.shape[1]), BF16),
        in_specs=vmem(3),
        out_specs=vmem(1)[0],
        name="norm",
    )(tokens, gain[None], leaks)


def slab_kernel(*refs):
    ins, o_ref = refs[:-1], refs[-1]
    start = pl.multiple_of(lax.axis_index("fs") * LANES, LANES)
    both = jnp.concatenate([w_ref[:, pl.ds(start, LANES)] for w_ref in ins], axis=1)
    for k in range(o_ref.shape[0]):
        o_ref[k] = both


def weight_slabs(weights, copies):
    rows = weights[0].shape[0]
    return pl.pallas_call(
        slab_kernel,
        out_shape=struct((copies, rows, len(weights) * LANES), BF16),
        in_specs=vmem(len(weights)),
        out_specs=vmem(1)[0],
        name="slab",
    )(*weights)


def relay_kernel(in_ref, early_ref, late_ref):
    early = in_ref[:, : 2 * LANES]
    for k in range(early_ref.shape[0]):
        early_ref[k] = early
    late_ref[...] = in_ref[:, 2 * LANES :]


def split_columns(rows, copies):
    deep, wide = rows.shape
    return pl.pallas_call(
        relay_kernel,
        out_shape=(
            struct((copies, deep, 2 * LANES), BF16),
            struct((deep, wide - 2 * LANES), BF16),
        ),
        in_specs=vmem(1),
        out_specs=tuple(vmem(2)),
        compiler_params=pltpu.CompilerParams(vmem_limit_bytes=4 << 20),
        name="relay",
    )(rows)


def place_rows(scratch, toks, r, w):
    core = lax.axis_index("tp")
    half = scratch.shape[0] // 2
    for part, place in ((2 * r, core), (2 * r + 1, 1 - core)):
        start = pl.multiple_of(place * half, half)
        scratch[pl.ds(start, half), :] = dot(toks[part, :half, :], w).astype(BF16)


def fetches(refs, toks, sems):
    return [pltpu.make_async_copy(ref, toks.at[k], sems.at[k]) for k, ref in enumerate(refs)]


def lower_triangle(n):
    row = lax.broadcasted_iota(jnp.int32, (n, n), 0)
    col = lax.broadcasted_iota(jnp.int32, (n, n), 1)
    return row >= col


def gates(logits, gap, tri):
    keys = gap * jax.nn.sigmoid(-logits.astype(F32))
    parts = dot(tri, jnp.concatenate(split_parts(jnp.log1p(-keys), 2), axis=1))
    return keys, parts[:, :LANES] + parts[:, LANES:]


def leak_row(toks, r, length):
    first = pl.multiple_of(lax.axis_index("fs") * length, LANES)
    coded = toks[2 * r, length // 2 :, pl.ds(first, length)].astype(F32)
    return jnp.sum(coded, axis=0, keepdims=True)


def state_kernel(*refs):
    tok_refs, rest = refs[:8], refs[8:]
    w_ref, floor_ref, state_ref, raw_ref, tail_ref, toks, sems, weights, w_sem = rest
    w_copy = pltpu.make_async_copy(w_ref, weights, w_sem)
    copies = fetches(tok_refs, toks, sems)
    for copy in [w_copy] + copies[:4]:
        copy.start()
    length = raw_ref.shape[1]
    tri = lower_triangle(length).astype(F32).astype(BF16)
    gap = 1.0 - floor_ref[...]
    lane = lax.broadcasted_iota(jnp.int32, (LANES, LANES), 1)
    w_copy.wait()
    w = weights[...]
    half = length // 2
    tails = []
    for r in range(4):
        copies[2 * r].wait()
        copies[2 * r + 1].wait()
        if r < 2:
            copies[2 * r + 4].start()
            copies[2 * r + 5].start()
        place_rows(raw_ref.at[r], toks, r, w)
        last_rows = [toks[2 * r + k, half - 16 : half, :].astype(F32)[8:] for k in range(2)]
        tails.append(jnp.where(lax.axis_index("tp") == 1, last_rows[0], last_rows[1]))
        keys, running = gates(raw_ref[r, :, :LANES], gap, tri)
        leaks = jnp.broadcast_to(leak_row(toks, r, length), (LANES, length))
        total = running + leaks.T
        last = total[length - 1 :, :]
        fading = (keys * jnp.exp(last - total)).astype(BF16)
        state = dot(fading, raw_ref[r, :, LANES:], ((0,), (0,)))
        spread = jnp.broadcast_to(last, (LANES, LANES)).T
        high = spread.astype(BF16).astype(F32)
        split = jnp.where(lane < LANES // 2, high, spread - high)
        packed = jnp.concatenate(
            [state.reshape(LANES // 8, 8, LANES), split.reshape(LANES // 8, 8, LANES)], axis=1
        )
        state_ref[r * 16 : (r + 1) * 16] = packed.astype(BF16)
    tail_ref[...] = jnp.concatenate(tails, axis=0).astype(BF16)


def anywhere(count):
    return [pl.BlockSpec(memory_space=pl.ANY) for _ in range(count)]


def token_scratch(tok, deep, columns):
    return [
        pltpu.VMEM((8, *tok.shape), BF16),
        pltpu.SemaphoreType.DMA((8,)),
        pltpu.VMEM((deep, columns), BF16),
        pltpu.SemaphoreType.DMA,
    ]


def local_states(toks, w, floor):
    length = 2 * (toks[0].shape[0] - 8)
    return pl.pallas_call(
        state_kernel,
        out_shape=(
            struct((64, 16, LANES), BF16),
            struct((4, length, 2 * LANES), BF16),
            struct((32, toks[0].shape[1]), BF16),
        ),
        in_specs=[*anywhere(9), *vmem(1)],
        out_specs=tuple(vmem(3)),
        scratch_shapes=token_scratch(toks[0], w.shape[0], 2 * LANES),
        name="states",
    )(*toks, w, floor)


def sequence_block(*dims):
    return pl.BlockSpec((1, *dims), lambda r: (r, 0, 0))


def whole(*dims):
    return pl.BlockSpec(dims, lambda r: (0,) * len(dims))


def scan_kernel(in_ref, o_ref):
    carry = jnp.zeros((8, LANES), F32)
    for k in range(in_ref.shape[0]):
        both = in_ref[k].astype(F32)
        o_ref[k] = carry.astype(BF16)
        coded = both[8:]
        decay = jnp.exp(coded + pltpu.roll(coded, LANES // 2, 1))
        carry = decay * carry + both[:8]


def scan_blocks(states):
    return pl.pallas_call(
        scan_kernel,
        out_shape=struct((states.shape[0], 8, LANES), BF16),
        in_specs=vmem(1),
        out_specs=vmem(1)[0],
        compiler_params=pltpu.CompilerParams(vmem_limit_bytes=4 << 20),
        name="scan",
    )(states)


def inside_kernel(*refs):
    tok_refs, rest = refs[:8], refs[8:]
    w_ref, floor_ref, early_ref, tail_ref, *rest = rest
    inside_ref, reach_ref, gate_ref, signal_ref, rim_ref, toks, sems, weights, w_sem, raw = rest
    w_copy = pltpu.make_async_copy(w_ref, weights, w_sem)
    copies = fetches(tok_refs, toks, sems)
    for copy in [w_copy] + copies[:4]:
        copy.start()
    length = early_ref.shape[1]
    causal = lower_triangle(length)
    tri = causal.astype(F32).astype(BF16)
    gap = 1.0 - floor_ref[...]
    w_copy.wait()
    w = weights[...]
    rim = dot(tail_ref[...], weights[:, 2 * LANES :]).astype(BF16).astype(F32)
    for r in range(4):
        rim_ref[r] = rim[8 * r : 8 * r + 8]
        keys, running = gates(early_ref[r, :, :LANES], gap, tri)
        copies[2 * r].wait()
        copies[2 * r + 1].wait()
        if r < 2:
            copies[2 * r + 4].start()
            copies[2 * r + 5].start()
        place_rows(raw, toks, r, w)
        gate_ref[r] = raw[:, LANES : 2 * LANES]
        signal_ref[r] = raw[:, 2 * LANES :]
        logits = raw[:, :LANES].astype(F32)
        query = logits * jax.nn.sigmoid(logits)
        middle = 0.5 * running[length - 1 :, :]
        ahead = (query * jnp.exp(running - middle)).astype(BF16)
        behind = (keys * jnp.exp(middle - running)).astype(BF16)
        leaks = leak_row(toks, r, length)
        columns = jnp.broadcast_to(leaks, (LANES, length)).T
        fade = jnp.exp(jnp.where(causal, columns[:, :1] - leaks, -jnp.inf))
        scores = dot(ahead, behind, ((1,), (1,))) * fade
        inside_ref[r] = dot(scores.astype(BF16), early_ref[r, :, LANES:])
        reach_ref[r] = (query * jnp.exp(running + columns)).astype(BF16)


def inside_blocks(toks, w, floor, early, tail):
    length = early.shape[1]
    block = (4, length, LANES)
    return pl.pallas_call(
        inside_kernel,
        out_shape=(
            struct(block, F32),
            struct(block, BF16),
            struct(block, BF16),
            struct(block, BF16),
            struct((4, 8, LANES), F32),
        ),
        in_specs=[*anywhere(9), *vmem(3)],
        out_specs=tuple(vmem(5)),
        scratch_shapes=[
            *token_scratch(toks[0], w.shape[0], 3 * LANES),
            pltpu.VMEM((length, 3 * LANES), BF16),
        ],
        name="inside",
    )(*toks, w, floor, early, tail)


def mix_kernel(
    inside_ref, reach_ref, state_ref, gate_ref, signal_ref, rim_ref, taps_ref, gain_ref, o_ref, padded
):
    length = inside_ref.shape[1]
    half = length // 2
    x = lax.axis_index("fs")
    r = pl.program_id(0)
    shift = jnp.where(r == 1, 3, jnp.where(r == 2, 1, jnp.where(r == 3, 2, 0)))
    sequence = (x + shift) % 4
    start = pl.multiple_of(x * LANES, LANES)
    taps = taps_ref[:, pl.ds(start, LANES)]
    padded[0:8, :] = rim_ref[0]
    padded[8:, :] = signal_ref[0].astype(F32)
    filtered = taps[0:1] * padded[6 : 6 + length, :]
    filtered = filtered + taps[1:2] * padded[7 : 7 + length, :]
    filtered = filtered + taps[2:3] * padded[8 : 8 + length, :]
    conv = (gate_ref[0].astype(F32) * filtered).astype(BF16)
    chain = inside_ref[0] + dot(reach_ref[0], state_ref[0])
    scale = lax.rsqrt(jnp.mean(chain * chain, axis=-1, keepdims=True) + 1e-06)
    chain = (chain * scale * gain_ref[...]).astype(BF16)
    for h in range(2):
        rows = slice(h * half, (h + 1) * half)
        o_ref[2 * sequence + h, :, :LANES] = conv[rows]
        o_ref[2 * sequence + h, :, LANES:] = chain[rows]


def mix_blocks(inside, reach, state, gate, signal, rim, taps, gain):
    length = inside.shape[1]
    narrow = sequence_block(length, LANES)
    return pl.pallas_call(
        mix_kernel,
        out_shape=struct((8, length // 2, 2 * LANES), BF16),
        grid=(4,),
        in_specs=[
            narrow,
            narrow,
            sequence_block(LANES, LANES),
            narrow,
            narrow,
            sequence_block(8, LANES),
            whole(*taps.shape),
            whole(1, LANES),
        ],
        out_specs=whole(8, length // 2, 2 * LANES),
        scratch_shapes=[pltpu.VMEM((length + 8, LANES), F32)],
        name="mix",
    )(inside, reach, state, gate, signal, rim, taps, gain)


def out_kernel(mix_ref, *refs):
    piece_refs, (o_ref, pieces, sems) = refs[:8], refs[8:]
    copies = [pltpu.make_async_copy(ref, pieces.at[k], sems.at[k]) for k, ref in enumerate(piece_refs)]
    for copy in copies[:4]:
        copy.start()
    core = lax.axis_index("tp")
    x = lax.axis_index("fs")
    rows = []
    for c in (core, 1 - core):
        parts = [mix_ref[2 * k + c] for k in range(4)]
        rows.append(
            jnp.concatenate(
                [part[:, :LANES] for part in parts] + [part[:, LANES:] for part in parts], axis=1
            )
        )
    wide = piece_refs[0].shape[1]
    for k in range(4):
        copies[2 * k].wait()
        copies[2 * k + 1].wait()
        if k < 2:
            copies[2 * k + 4].start()
            copies[2 * k + 5].start()
        start = pl.multiple_of((x + SLOT_SHIFT[k]) % 4 * wide, wide)
        total = dot(rows[0], pieces[2 * k]) + dot(rows[1], pieces[2 * k + 1])
        o_ref[:, pl.ds(start, wide)] = total.astype(BF16)


def out_rows(mix, nears, fars):
    rows = mix.shape[1]
    deep, wide = nears[0].shape
    pieces = [piece for pair in zip(nears, fars) for piece in pair]
    return pl.pallas_call(
        out_kernel,
        out_shape=struct((rows, 4 * wide), BF16),
        in_specs=[*vmem(1), *anywhere(8)],
        out_specs=vmem(1)[0],
        scratch_shapes=[pltpu.VMEM((8, deep, wide), BF16), pltpu.SemaphoreType.DMA((8,))],
        name="out",
    )(mix, *pieces)


def ring(array, axis, by):
    count = lax.axis_size(axis)
    return lax.ppermute(array, axis, [(i, (i + by) % count) for i in range(count)])


def exchanged(array, axis):
    return lax.all_to_all(array, axis, split_axis=0, concat_axis=0, tiled=True)


def layer(
    tokens,
    norm_gain,
    conv_gate_w,
    conv_in_w,
    query_w,
    forget_w,
    value_w,
    conv_taps,
    floor_gate,
    leak,
    head_gain,
    conv_out_w,
    chain_out_w,
):
    x = lax.axis_index("fs")
    slabs = weight_slabs((forget_w, value_w, query_w, conv_gate_w, conv_in_w), 8)
    y_rows = exchanged(slabs, "sp_1").reshape(-1, slabs.shape[2])
    early, late = split_columns(y_rows, 8)
    early_w = exchanged(early, "sp_0").reshape(-1, early.shape[2])
    late_w = lax.all_gather(late, "sp_0", axis=0, tiled=True)

    own = norm_rows(tokens[0], norm_gain, leak[0].T)
    near = [own]
    for by in (1, 3, 2):
        near.append(ring(own, "fs", by))
    far = []
    for part in near:
        far.append(ring(part, "tp", 1))
    toks = [part for pair in zip(near, far) for part in pair]

    out_w = jnp.concatenate([conv_out_w, chain_out_w], axis=0)
    out_near = [out_w]
    for by in (1, 3, 2):
        out_near.append(ring(out_w, "fs", by))
    out_far = []
    for part in out_near:
        out_far.append(ring(part, "tp", 1))

    floor = lax.dynamic_slice_in_dim(floor_gate, x * LANES, LANES, 0)[None]
    states, projected, tail = local_states(toks, early_w, floor)
    arrived = exchanged(states, SP)
    before = exchanged(scan_blocks(arrived), SP)
    before = before.reshape(4, LANES, LANES)

    count = 64
    tail = lax.ppermute(tail, SP, [(i, i + 1) for i in range(count - 1)])
    inside, reach, gate, signal, rim = inside_blocks(toks, late_w, floor, projected, tail)
    mix = mix_blocks(inside, reach, before, gate, signal, rim, conv_taps, head_gain[None])
    mix = exchanged(mix, ("fs", "tp"))
    return out_rows(mix, out_near, out_far)[None]


def solution(mesh):
    split = Mesh(
        mesh.devices.reshape(8, 8, mesh.shape["fs"], mesh.shape["tp"]), ("sp_0", "sp_1", "fs", "tp")
    )
    in_specs = (
        P("fs", SP_TP, None),
        P(),
        P(SP, "tp"),
        P(SP, "tp"),
        P(SP, "tp"),
        P(SP, "tp"),
        P(SP, "tp"),
        P(None, "tp"),
        P("tp"),
        P("fs", SP, "tp"),
        P(),
        P("tp", "fs"),
        P("tp", "fs"),
    )
    out_specs = P("fs", SP_TP, None)
    return jax.shard_map(layer, mesh=split, in_specs=in_specs, out_specs=out_specs, check_vma=False)
```

```python
import jax
import jax.numpy as jnp
from jax import lax
from jax.experimental import pallas as pl
from jax.experimental.pallas import tpu as pltpu
from jax.sharding import Mesh
from jax.sharding import PartitionSpec as P

SP = ("sp_0", "sp_1")
SP_TP = ("sp_0", "sp_1", "tp")
F32 = jnp.float32
BF16 = jnp.bfloat16
LANES = 128
SLOT_SHIFT = (0, 3, 1, 2)


def struct(shape, dtype):
    return jax.ShapeDtypeStruct(shape, dtype)


def vmem(count):
    return [pl.BlockSpec(memory_space=pltpu.VMEM) for _ in range(count)]


def split_parts(values, count):
    parts = []
    for _ in range(count):
        parts.append(values.astype(BF16))
        values = values - parts[-1].astype(F32)
    return parts


def dot(a, b, dims=((1,), (0,))):
    return lax.dot_general(a, b, (dims, ((), ())), preferred_element_type=F32)


def norm_kernel(x_ref, gain_ref, leak_ref, o_ref):
    rows = x_ref.shape[0]
    values = x_ref[...].astype(F32)
    center = values - jnp.mean(values, axis=-1, keepdims=True)
    spread = jnp.mean(center * center, axis=-1, keepdims=True)
    o_ref[:rows, :] = (center * lax.rsqrt(spread + 1e-05) * gain_ref[...]).astype(BF16)
    heads, length = leak_ref.shape
    parts = [part.astype(F32) for part in split_parts(leak_ref[...], 3)]
    both = jnp.concatenate([*parts, jnp.zeros_like(parts[0])], axis=0).astype(BF16)
    ahead = lax.broadcasted_iota(jnp.int32, (length, length), 0)
    here = lax.broadcasted_iota(jnp.int32, (length, length), 1)
    sums = dot(both, (ahead <= here).astype(F32).astype(BF16))
    total = sums[:heads] + sums[heads : 2 * heads] + sums[2 * heads : 3 * heads]
    leaks = jnp.concatenate([total[h : h + 1, :] for h in range(heads)], axis=1)
    parts = [part.astype(F32) for part in split_parts(leaks, 3)]
    tail = jnp.concatenate([*parts, jnp.zeros((8 - len(parts), leaks.shape[1]), F32)], axis=0)
    unused = jnp.zeros((8, o_ref.shape[1] - leaks.shape[1]), F32)
    o_ref[rows:, :] = jnp.concatenate([tail, unused], axis=1).astype(BF16)


def norm_rows(tokens, gain, leaks):
    return pl.pallas_call(
        norm_kernel,
        out_shape=struct((tokens.shape[0] + 8, tokens.shape[1]), BF16),
        in_specs=vmem(3),
        out_specs=vmem(1)[0],
        name="norm",
    )(tokens, gain[None], leaks)


def slab_kernel(*refs):
    ins, o_ref = refs[:-1], refs[-1]
    start = pl.multiple_of(lax.axis_index("fs") * LANES, LANES)
    both = jnp.concatenate([w_ref[:, pl.ds(start, LANES)] for w_ref in ins], axis=1)
    for k in range(o_ref.shape[0]):
        o_ref[k] = both


def weight_slabs(weights, copies):
    rows = weights[0].shape[0]
    return pl.pallas_call(
        slab_kernel,
        out_shape=struct((copies, rows, len(weights) * LANES), BF16),
        in_specs=vmem(len(weights)),
        out_specs=vmem(1)[0],
        name="slab",
    )(*weights)


def relay_kernel(in_ref, early_ref, late_ref):
    early = in_ref[:, : 2 * LANES]
    for k in range(early_ref.shape[0]):
        early_ref[k] = early
    late_ref[...] = in_ref[:, 2 * LANES :]


def split_columns(rows, copies):
    deep, wide = rows.shape
    return pl.pallas_call(
        relay_kernel,
        out_shape=(
            struct((copies, deep, 2 * LANES), BF16),
            struct((deep, wide - 2 * LANES), BF16),
        ),
        in_specs=vmem(1),
        out_specs=tuple(vmem(2)),
        compiler_params=pltpu.CompilerParams(vmem_limit_bytes=4 << 20),
        name="relay",
    )(rows)


def place_rows(scratch, toks, r, w):
    core = lax.axis_index("tp")
    half = scratch.shape[0] // 2
    for part, place in ((2 * r, core), (2 * r + 1, 1 - core)):
        start = pl.multiple_of(place * half, half)
        scratch[pl.ds(start, half), :] = dot(toks[part, :half, :], w).astype(BF16)


def fetches(refs, toks, sems):
    return [pltpu.make_async_copy(ref, toks.at[k], sems.at[k]) for k, ref in enumerate(refs)]


def lower_triangle(n):
    row = lax.broadcasted_iota(jnp.int32, (n, n), 0)
    col = lax.broadcasted_iota(jnp.int32, (n, n), 1)
    return row >= col


def gates(logits, gap, tri):
    keys = gap * jax.nn.sigmoid(-logits.astype(F32))
    parts = dot(tri, jnp.concatenate(split_parts(jnp.log1p(-keys), 2), axis=1))
    return keys, parts[:, :LANES] + parts[:, LANES:]


def leak_row(toks, r, length):
    first = pl.multiple_of(lax.axis_index("fs") * length, LANES)
    coded = toks[2 * r, length // 2 :, pl.ds(first, length)].astype(F32)
    return jnp.sum(coded, axis=0, keepdims=True)


def state_kernel(*refs):
    tok_refs, rest = refs[:8], refs[8:]
    w_ref, floor_ref, state_ref, raw_ref, tail_ref, toks, sems, weights, w_sem = rest
    w_copy = pltpu.make_async_copy(w_ref, weights, w_sem)
    copies = fetches(tok_refs, toks, sems)
    for copy in [w_copy] + copies[:4]:
        copy.start()
    length = raw_ref.shape[1]
    tri = lower_triangle(length).astype(F32).astype(BF16)
    gap = 1.0 - floor_ref[...]
    lane = lax.broadcasted_iota(jnp.int32, (LANES, LANES), 1)
    w_copy.wait()
    w = weights[...]
    half = length // 2
    tails = []
    for r in range(4):
        copies[2 * r].wait()
        copies[2 * r + 1].wait()
        if r < 2:
            copies[2 * r + 4].start()
            copies[2 * r + 5].start()
        place_rows(raw_ref.at[r], toks, r, w)
        last_rows = [toks[2 * r + k, half - 16 : half, :].astype(F32)[8:] for k in range(2)]
        tails.append(jnp.where(lax.axis_index("tp") == 1, last_rows[0], last_rows[1]))
        keys, running = gates(raw_ref[r, :, :LANES], gap, tri)
        leaks = jnp.broadcast_to(leak_row(toks, r, length), (LANES, length))
        total = running + leaks.T
        last = total[length - 1 :, :]
        fading = (keys * jnp.exp(last - total)).astype(BF16)
        state = dot(fading, raw_ref[r, :, LANES:], ((0,), (0,)))
        spread = jnp.broadcast_to(last, (LANES, LANES)).T
        high = spread.astype(BF16).astype(F32)
        split = jnp.where(lane < LANES // 2, high, spread - high)
        packed = jnp.concatenate(
            [state.reshape(LANES // 8, 8, LANES), split.reshape(LANES // 8, 8, LANES)], axis=1
        )
        state_ref[r * 16 : (r + 1) * 16] = packed.astype(BF16)
    tail_ref[...] = jnp.concatenate(tails, axis=0).astype(BF16)


def anywhere(count):
    return [pl.BlockSpec(memory_space=pl.ANY) for _ in range(count)]


def token_scratch(tok, deep, columns):
    return [
        pltpu.VMEM((8, *tok.shape), BF16),
        pltpu.SemaphoreType.DMA((8,)),
        pltpu.VMEM((deep, columns), BF16),
        pltpu.SemaphoreType.DMA,
    ]


def local_states(toks, w, floor):
    length = 2 * (toks[0].shape[0] - 8)
    return pl.pallas_call(
        state_kernel,
        out_shape=(
            struct((64, 16, LANES), BF16),
            struct((4, length, 2 * LANES), BF16),
            struct((32, toks[0].shape[1]), BF16),
        ),
        in_specs=[*anywhere(9), *vmem(1)],
        out_specs=tuple(vmem(3)),
        scratch_shapes=token_scratch(toks[0], w.shape[0], 2 * LANES),
        name="states",
    )(*toks, w, floor)


def sequence_block(*dims):
    return pl.BlockSpec((1, *dims), lambda r: (r, 0, 0))


def whole(*dims):
    return pl.BlockSpec(dims, lambda r: (0,) * len(dims))


def scan_kernel(in_ref, o_ref):
    carry = jnp.zeros((8, LANES), F32)
    for k in range(in_ref.shape[0]):
        both = in_ref[k].astype(F32)
        o_ref[k] = carry.astype(BF16)
        coded = both[8:]
        decay = jnp.exp(coded + pltpu.roll(coded, LANES // 2, 1))
        carry = decay * carry + both[:8]


def scan_blocks(states):
    return pl.pallas_call(
        scan_kernel,
        out_shape=struct((states.shape[0], 8, LANES), BF16),
        in_specs=vmem(1),
        out_specs=vmem(1)[0],
        compiler_params=pltpu.CompilerParams(vmem_limit_bytes=4 << 20),
        name="scan",
    )(states)


def prepare_kernel(floor_ref, early_ref, run_ref, behind_ref):
    length = early_ref.shape[1]
    tri = lower_triangle(length).astype(F32).astype(BF16)
    keys, running = gates(early_ref[0, :, :LANES], 1.0 - floor_ref[...], tri)
    middle = 0.5 * running[length - 1 :, :]
    behind_ref[0] = (keys * jnp.exp(middle - running)).astype(BF16)
    run_ref[0] = running


def prepared(floor, early):
    length = early.shape[1]
    block = (4, length, LANES)
    narrow = sequence_block(length, LANES)
    return pl.pallas_call(
        prepare_kernel,
        out_shape=(struct(block, F32), struct(block, BF16)),
        grid=(4,),
        in_specs=[whole(1, LANES), sequence_block(length, 2 * LANES)],
        out_specs=(narrow, narrow),
        name="prepare",
    )(floor, early)


def inside_kernel(*refs):
    tok_refs, rest = refs[:8], refs[8:]
    w_ref, early_ref, run_ref, behind_ref, tail_ref, *rest = rest
    inside_ref, reach_ref, gate_ref, signal_ref, rim_ref, toks, sems, weights, w_sem, raw = rest
    w_copy = pltpu.make_async_copy(w_ref, weights, w_sem)
    copies = fetches(tok_refs, toks, sems)
    for copy in [w_copy] + copies[:4]:
        copy.start()
    length = early_ref.shape[1]
    causal = lower_triangle(length)
    w_copy.wait()
    w = weights[...]
    rim = dot(tail_ref[...], weights[:, 2 * LANES :]).astype(BF16).astype(F32)
    for r in range(4):
        rim_ref[r] = rim[8 * r : 8 * r + 8]
        running = run_ref[r]
        copies[2 * r].wait()
        copies[2 * r + 1].wait()
        if r < 2:
            copies[2 * r + 4].start()
            copies[2 * r + 5].start()
        place_rows(raw, toks, r, w)
        gate_ref[r] = raw[:, LANES : 2 * LANES]
        signal_ref[r] = raw[:, 2 * LANES :]
        logits = raw[:, :LANES].astype(F32)
        query = logits * jax.nn.sigmoid(logits)
        middle = 0.5 * running[length - 1 :, :]
        ahead = (query * jnp.exp(running - middle)).astype(BF16)
        leaks = leak_row(toks, r, length)
        columns = jnp.broadcast_to(leaks, (LANES, length)).T
        fade = jnp.exp(jnp.where(causal, columns[:, :1] - leaks, -jnp.inf))
        scores = dot(ahead, behind_ref[r], ((1,), (1,))) * fade
        inside_ref[r] = dot(scores.astype(BF16), early_ref[r, :, LANES:])
        reach_ref[r] = (query * jnp.exp(running + columns)).astype(BF16)


def inside_blocks(toks, w, early, running, behind, tail):
    length = early.shape[1]
    block = (4, length, LANES)
    return pl.pallas_call(
        inside_kernel,
        out_shape=(
            struct(block, F32),
            struct(block, BF16),
            struct(block, BF16),
            struct(block, BF16),
            struct((4, 8, LANES), F32),
        ),
        in_specs=[*anywhere(9), *vmem(4)],
        out_specs=tuple(vmem(5)),
        scratch_shapes=[
            *token_scratch(toks[0], w.shape[0], 3 * LANES),
            pltpu.VMEM((length, 3 * LANES), BF16),
        ],
        name="inside",
    )(*toks, w, early, running, behind, tail)


def mix_kernel(
    inside_ref, reach_ref, state_ref, gate_ref, signal_ref, rim_ref, taps_ref, gain_ref, o_ref, padded
):
    length = inside_ref.shape[1]
    half = length // 2
    x = lax.axis_index("fs")
    r = pl.program_id(0)
    shift = jnp.where(r == 1, 3, jnp.where(r == 2, 1, jnp.where(r == 3, 2, 0)))
    sequence = (x + shift) % 4
    start = pl.multiple_of(x * LANES, LANES)
    taps = taps_ref[:, pl.ds(start, LANES)]
    padded[0:8, :] = rim_ref[0]
    padded[8:, :] = signal_ref[0].astype(F32)
    filtered = taps[0:1] * padded[6 : 6 + length, :]
    filtered = filtered + taps[1:2] * padded[7 : 7 + length, :]
    filtered = filtered + taps[2:3] * padded[8 : 8 + length, :]
    conv = (gate_ref[0].astype(F32) * filtered).astype(BF16)
    chain = inside_ref[0] + dot(reach_ref[0], state_ref[0])
    scale = lax.rsqrt(jnp.mean(chain * chain, axis=-1, keepdims=True) + 1e-06)
    chain = (chain * scale * gain_ref[...]).astype(BF16)
    for h in range(2):
        rows = slice(h * half, (h + 1) * half)
        o_ref[2 * sequence + h, :, :LANES] = conv[rows]
        o_ref[2 * sequence + h, :, LANES:] = chain[rows]


def mix_blocks(inside, reach, state, gate, signal, rim, taps, gain):
    length = inside.shape[1]
    narrow = sequence_block(length, LANES)
    return pl.pallas_call(
        mix_kernel,
        out_shape=struct((8, length // 2, 2 * LANES), BF16),
        grid=(4,),
        in_specs=[
            narrow,
            narrow,
            sequence_block(LANES, LANES),
            narrow,
            narrow,
            sequence_block(8, LANES),
            whole(*taps.shape),
            whole(1, LANES),
        ],
        out_specs=whole(8, length // 2, 2 * LANES),
        scratch_shapes=[pltpu.VMEM((length + 8, LANES), F32)],
        name="mix",
    )(inside, reach, state, gate, signal, rim, taps, gain)


def out_kernel(mix_ref, *refs):
    piece_refs, (o_ref, pieces, sems) = refs[:8], refs[8:]
    copies = [pltpu.make_async_copy(ref, pieces.at[k], sems.at[k]) for k, ref in enumerate(piece_refs)]
    for copy in copies[:4]:
        copy.start()
    core = lax.axis_index("tp")
    x = lax.axis_index("fs")
    rows = []
    for c in (core, 1 - core):
        parts = [mix_ref[2 * k + c] for k in range(4)]
        rows.append(
            jnp.concatenate(
                [part[:, :LANES] for part in parts] + [part[:, LANES:] for part in parts], axis=1
            )
        )
    wide = piece_refs[0].shape[1]
    for k in range(4):
        copies[2 * k].wait()
        copies[2 * k + 1].wait()
        if k < 2:
            copies[2 * k + 4].start()
            copies[2 * k + 5].start()
        start = pl.multiple_of((x + SLOT_SHIFT[k]) % 4 * wide, wide)
        total = dot(rows[0], pieces[2 * k]) + dot(rows[1], pieces[2 * k + 1])
        o_ref[:, pl.ds(start, wide)] = total.astype(BF16)


def out_rows(mix, nears, fars):
    rows = mix.shape[1]
    deep, wide = nears[0].shape
    pieces = [piece for pair in zip(nears, fars) for piece in pair]
    return pl.pallas_call(
        out_kernel,
        out_shape=struct((rows, 4 * wide), BF16),
        in_specs=[*vmem(1), *anywhere(8)],
        out_specs=vmem(1)[0],
        scratch_shapes=[pltpu.VMEM((8, deep, wide), BF16), pltpu.SemaphoreType.DMA((8,))],
        name="out",
    )(mix, *pieces)


def ring(array, axis, by):
    count = lax.axis_size(axis)
    return lax.ppermute(array, axis, [(i, (i + by) % count) for i in range(count)])


def exchanged(array, axis):
    return lax.all_to_all(array, axis, split_axis=0, concat_axis=0, tiled=True)


def layer(
    tokens,
    norm_gain,
    conv_gate_w,
    conv_in_w,
    query_w,
    forget_w,
    value_w,
    conv_taps,
    floor_gate,
    leak,
    head_gain,
    conv_out_w,
    chain_out_w,
):
    x = lax.axis_index("fs")
    slabs = weight_slabs((forget_w, value_w, query_w, conv_gate_w, conv_in_w), 8)
    y_rows = exchanged(slabs, "sp_1").reshape(-1, slabs.shape[2])
    early, late = split_columns(y_rows, 8)
    early_w = exchanged(early, "sp_0").reshape(-1, early.shape[2])
    late_w = lax.all_gather(late, "sp_0", axis=0, tiled=True)

    own = norm_rows(tokens[0], norm_gain, leak[0].T)
    near = [own]
    for by in (1, 3, 2):
        near.append(ring(own, "fs", by))
    far = []
    for part in near:
        far.append(ring(part, "tp", 1))
    toks = [part for pair in zip(near, far) for part in pair]

    out_w = jnp.concatenate([conv_out_w, chain_out_w], axis=0)
    out_near = [out_w]
    for by in (1, 3, 2):
        out_near.append(ring(out_w, "fs", by))
    out_far = []
    for part in out_near:
        out_far.append(ring(part, "tp", 1))

    floor = lax.dynamic_slice_in_dim(floor_gate, x * LANES, LANES, 0)[None]
    states, projected, tail = local_states(toks, early_w, floor)
    arrived = exchanged(states, SP)
    before = exchanged(scan_blocks(arrived), SP)
    before = before.reshape(4, LANES, LANES)

    count = 64
    tail = lax.ppermute(tail, SP, [(i, i + 1) for i in range(count - 1)])
    running, behind = prepared(floor, projected)
    inside, reach, gate, signal, rim = inside_blocks(toks, late_w, projected, running, behind, tail)
    mix = mix_blocks(inside, reach, before, gate, signal, rim, conv_taps, head_gain[None])
    mix = exchanged(mix, ("fs", "tp"))
    return out_rows(mix, out_near, out_far)[None]


def solution(mesh):
    split = Mesh(
        mesh.devices.reshape(8, 8, mesh.shape["fs"], mesh.shape["tp"]), ("sp_0", "sp_1", "fs", "tp")
    )
    in_specs = (
        P("fs", SP_TP, None),
        P(),
        P(SP, "tp"),
        P(SP, "tp"),
        P(SP, "tp"),
        P(SP, "tp"),
        P(SP, "tp"),
        P(None, "tp"),
        P("tp"),
        P("fs", SP, "tp"),
        P(),
        P("tp", "fs"),
        P("tp", "fs"),
    )
    out_specs = P("fs", SP_TP, None)
    return jax.shard_map(layer, mesh=split, in_specs=in_specs, out_specs=out_specs, check_vma=False)
```
